32 devices in a mesh: sp: 8 (over z, y), tp: 4 (over x, core).
Axes of the slice: x: 2, y: 2, z: 4, core: 2. Of those that a mesh axis runs over, the one named last changes fastest.
Arguments:
- query: bfloat16 [12288, 512], P('sp', 'tp'), may hold values from -6 to 6
- key_rows: bfloat16 [12288, 512], P('sp', 'tp'), may hold values from -6 to 6
- value: bfloat16 [12288, 1024], P('sp', 'tp'), may hold values from -6 to 6
- in_gate: float32 [2, 8, 12288], P(None, 'tp', 'sp'), may hold values from -6 to 250
- forget_pre: float32 [2, 8, 12288], P(None, 'tp', 'sp'), may hold values from 0.3 to 12
- out_gate: bfloat16 [12288, 1024], P('sp', 'tp'), may hold values from -6 to 6
- head_gain: bfloat16 [1024], P('tp'), may hold values from 0.099609375 to 1.8984375
- out_weight: bfloat16 [1024, 2048], P('tp'), may hold values from -0.25 to 0.25
- stream: bfloat16 [12288, 2048], P('sp', 'tp'), may hold values from -16 to 16
- norm_gain: bfloat16 [2048], P('tp'), may hold values from 0.099609375 to 1.8984375
- gate_weight: bfloat16 [2048, 5632], P('sp', 'tp'), may hold values from -0.125 to 0.125
- up_weight: bfloat16 [2048, 5632], P('sp', 'tp'), may hold values from -0.125 to 0.125
- down_weight: bfloat16 [2048, 5632], P('sp', 'tp'), may hold values from -0.109375 to 0.109375
Outputs:
- layer_out: bfloat16 [12288, 2048], P('sp', 'tp')
The draws below stay inside these ranges and needn't reach their ends.
All inputs are finite; a program needn't handle non-finite values.
Results may differ from the reference program's by a relative error of at most 0.04.
Values may be sent and summed in bfloat16 or wider, within the bound.
A program may use at most 128 MiB of HBM per device.

```python
import jax
import jax.numpy as jnp
from jax import lax

D = 2048
MEMORY_HEADS = 8
DK = 64
DV = 128
FF = 5632
BLOCK = 128
TOK_DEV = 1536
SEQUENCE_TOKENS = 12288
N_TP = 4


def draw_in_gate(key, part):
    random_subkeys = jax.random.split(jax.random.fold_in(key, 11), 1)
    return jnp.clip(1.5 * jax.random.normal(random_subkeys[0], (2, MEMORY_HEADS, SEQUENCE_TOKENS), jnp.float32), -6.0, 6.0)


def draw_forget_pre(key, part):
    random_subkeys = jax.random.split(jax.random.fold_in(key, 23), 5)
    slow_share = 0.5
    slow = jax.random.uniform(random_subkeys[0], (2, MEMORY_HEADS, 1), jnp.float32) < slow_share
    spans = SEQUENCE_TOKENS // TOK_DEV
    factor = jnp.exp(jax.random.uniform(random_subkeys[1], (2, MEMORY_HEADS, spans), jnp.float32, -0.6931, 0.6931))
    factor = jnp.repeat(factor, TOK_DEV, axis=2)
    noise = 0.7 * jnp.clip(jax.random.normal(random_subkeys[2], (2, MEMORY_HEADS, SEQUENCE_TOKENS), jnp.float32), -2.5, 2.5)
    slow_pre = jnp.log(SEQUENCE_TOKENS / (0.6 * factor)) + noise
    fast_pre = jnp.log(50.0 / factor) + noise
    final_output = jnp.clip(jnp.where(slow, slow_pre, fast_pre), 0.3, 12.0)
    spike_list = jax.random.randint(random_subkeys[3], (2, MEMORY_HEADS, 3), 0, SEQUENCE_TOKENS)
    token_offset = jnp.arange(SEQUENCE_TOKENS)[None, None, None, :]
    flagged_entries = jnp.any(token_offset == spike_list[..., None], axis=2)
    spike_value = jax.random.uniform(random_subkeys[4], (2, MEMORY_HEADS, SEQUENCE_TOKENS), jnp.float32, 0.3, 1.5)
    return jnp.where(flagged_entries, spike_value, final_output)


def draw_stream(key, part):
    random_subkeys = jax.random.split(jax.random.fold_in(key, 37), 2)
    columns = jnp.arange(D, dtype=jnp.float32) / D
    rowdraw = jax.random.uniform(random_subkeys[1], (SEQUENCE_TOKENS, 1), jnp.float32)
    base = jnp.clip(jax.random.normal(random_subkeys[0], (SEQUENCE_TOKENS, D), jnp.float32), -4.0, 4.0)
    column_scale = jnp.exp(jnp.log(4.0) * (columns - 0.5))
    row_scale = jnp.exp(jnp.log(10.0) * (rowdraw - 0.7))
    return (base * row_scale * column_scale[None, :]).astype(jnp.bfloat16)


def raised(drawn, key, source, target, blocks, factor):
    def block_of(axis_at):
        return (jnp.arange(drawn.shape[axis_at]) // (drawn.shape[axis_at] // blocks)).reshape((-1,) + (1,) * (drawn.ndim - 1 - axis_at))

    first = jax.random.permutation(key, blocks)[block_of(target)]
    second = (block_of(target) + blocks // 2) % blocks
    return jnp.where((block_of(source) == first) | (block_of(source) == second), factor * drawn, drawn)


def block_scale(own_key, shape, cuts, least, largest):
    gain = 1.0
    for dim, blocks in cuts:
        draws = jax.random.uniform(jax.random.fold_in(jax.random.fold_in(own_key, 6), dim), (blocks,), jnp.float32, least / len(cuts), largest / len(cuts))
        gain = gain * jnp.repeat(jnp.exp(draws), shape[dim] // blocks).reshape((-1,) + (1,) * (len(shape) - 1 - dim))
    return gain


def scatter_about(rng, shape, scale, reach, cuts=(), kind=jnp.bfloat16):
    values = jax.random.normal(rng, shape, jnp.float32) * scale
    if len(cuts) > 0:
        values = block_scale(rng, shape, cuts, -0.22, 0.18) * values
    return jnp.clip(values, min=-reach, max=reach).astype(kind)


def gaussian_with(own_key, extent, spread, most, shards, heavy, held_as=jnp.bfloat16):
    values = spread * jax.random.normal(own_key, extent, jnp.float32)
    if shards:
        values = values * block_scale(own_key, extent, shards, -0.22, 0.18)
    return jnp.clip(raised(values, jax.random.fold_in(own_key, 3), *heavy), -most, most).astype(held_as)


def setup_inputs(seed: int = 0) -> dict:
    arg_keys = jax.random.split(jax.random.key(seed), 14)
    return {
        "query": scatter_about(arg_keys[0], (SEQUENCE_TOKENS, MEMORY_HEADS * DK), 1.0, 6.0, ((0, 8), (1, 4))),
        "key_rows": scatter_about(arg_keys[1], (SEQUENCE_TOKENS, MEMORY_HEADS * DK), 1.0, 6.0, ((0, 8), (1, 4))),
        "value": scatter_about(arg_keys[2], (SEQUENCE_TOKENS, MEMORY_HEADS * DV), 1.0, 6.0, ((0, 8), (1, 4))),
        "in_gate": draw_in_gate(jax.random.fold_in(arg_keys[13], 71), 0),
        "forget_pre": draw_forget_pre(jax.random.fold_in(arg_keys[13], 71), 0),
        "out_gate": scatter_about(arg_keys[5], (SEQUENCE_TOKENS, MEMORY_HEADS * DV), 1.5, 6.0, ((0, 8), (1, 4))),
        "head_gain": jnp.clip(1.0 + 0.18 * jax.random.normal(arg_keys[6], (MEMORY_HEADS * DV,), jnp.float32), 0.099609375, 1.8984375).astype(jnp.bfloat16),
        "out_weight": gaussian_with(arg_keys[7], (MEMORY_HEADS * DV, D), (MEMORY_HEADS * DV) ** -0.5, 0.25, ((0, 4),), (0, 1, 4, 2.0)),
        "stream": draw_stream(jax.random.fold_in(arg_keys[13], 71), 0),
        "norm_gain": jnp.clip(1.0 + 0.18 * jax.random.normal(arg_keys[9], (D,), jnp.float32), 0.099609375, 1.8984375).astype(jnp.bfloat16),
        "gate_weight": scatter_about(arg_keys[10], (D, FF), D ** -0.5, 0.125, ((0, 8), (1, 4))),
        "up_weight": scatter_about(arg_keys[11], (D, FF), D ** -0.5, 0.125, ((0, 8), (1, 4))),
        "down_weight": gaussian_with(arg_keys[12], (D, FF), FF ** -0.5, 0.109375, ((0, 8), (1, 4)), (1, 0, 8, 2.0)),
    }


HIGHEST = lax.Precision.HIGHEST
EPSILON = 1e-06

def direction(queries, keys, values, input_gates, forgets):
    head_count = queries.shape[0]
    block_count = queries.shape[1] // BLOCK

    def blocks(item):
        shaped = item.reshape((head_count, block_count, BLOCK) + item.shape[2:])
        return jnp.moveaxis(shaped, 1, 0)
    causal = jnp.tril(jnp.ones((BLOCK, BLOCK), dtype=bool))

    def step(carry, pieces):
        matrix, normer, stable = carry
        query_part, key_part, value_part, gate_part, forget_part = pieces
        cumulative = jnp.cumsum(forget_part, axis=-1)
        decay_log = jnp.where(causal, cumulative[:, :, None] - cumulative[:, None, :] + gate_part[:, None, :], -jnp.inf)
        carry_log = cumulative + stable[:, None]
        row_peak = jnp.maximum(carry_log, lax.optimization_barrier(jnp.max(decay_log, axis=-1)))
        scores = jnp.einsum('hjd,hsd->hjs', query_part, key_part, precision=HIGHEST) * jnp.exp(decay_log - row_peak[:, :, None])
        carried = jnp.exp(carry_log - row_peak)
        numerator = jnp.einsum('hjs,hsv->hjv', scores, value_part, precision=HIGHEST) + carried[:, :, None] * jnp.einsum('hvd,hjd->hjv', matrix, query_part, precision=HIGHEST)
        denominator = lax.optimization_barrier(jnp.sum(scores, axis=-1)) + carried * jnp.einsum('hd,hjd->hj', normer, query_part, precision=HIGHEST)
        output = numerator / jnp.maximum(jnp.abs(denominator), jnp.exp(-row_peak))[:, :, None]
        block_total = cumulative[:, -1]
        weight_log = block_total[:, None] - cumulative + gate_part
        new_stable = jnp.maximum(block_total + stable, lax.optimization_barrier(jnp.max(weight_log, axis=-1)))
        shrink = jnp.exp(block_total + stable - new_stable)
        weight = jnp.exp(weight_log - new_stable[:, None])
        new_matrix = shrink[:, None, None] * matrix + jnp.einsum('hsv,hsd->hvd', weight[:, :, None] * value_part, key_part, precision=HIGHEST)
        new_normer = shrink[:, None] * normer + jnp.einsum('hs,hsd->hd', weight, key_part, precision=HIGHEST)
        return ((new_matrix, new_normer, new_stable), output)
    initial = (jnp.zeros((head_count, values.shape[2], queries.shape[2]), jnp.float32), jnp.zeros((head_count, queries.shape[2]), jnp.float32), jnp.zeros((head_count,), jnp.float32))
    _, results = lax.scan(step, initial, (blocks(queries), blocks(keys), blocks(values), blocks(input_gates), blocks(forgets)))
    return jnp.moveaxis(results, 0, 1).reshape(head_count, -1, values.shape[2])

def reverse_time(item):
    return jnp.flip(item, axis=1)

def reference(query, key_rows, value, in_gate, forget_pre, out_gate, head_gain, out_weight, stream, norm_gain, gate_weight, up_weight, down_weight):
    length = query.shape[0]

    def split_heads(item, width):
        return jnp.transpose(item.astype(jnp.float32).reshape(length, MEMORY_HEADS, width), (1, 0, 2))
    queries = split_heads(query, DK) * DK ** (-0.5)
    keys = split_heads(key_rows, DK)
    values = split_heads(value, DV)
    gates_in = in_gate.astype(jnp.float32)
    forgets = jax.nn.log_sigmoid(forget_pre.astype(jnp.float32))
    forward = direction(queries, keys, values, gates_in[0], forgets[0])
    backward = reverse_time(direction(reverse_time(queries), reverse_time(keys), reverse_time(values), reverse_time(gates_in[1]), reverse_time(forgets[1])))
    summed = forward + backward
    head_normed = summed * lax.rsqrt(lax.optimization_barrier(jnp.mean(summed * summed, axis=-1, keepdims=True)) + EPSILON)
    merged = jnp.transpose(head_normed, (1, 0, 2)).reshape(length, MEMORY_HEADS * DV)
    gated = (merged * head_gain.astype(jnp.float32) * jax.nn.sigmoid(out_gate.astype(jnp.float32))).astype(jnp.bfloat16)
    group_width = MEMORY_HEADS * DV // N_TP
    mixed_sum = jnp.zeros((length, D), jnp.float32)
    for group_index in range(N_TP):
        lower = group_index * group_width
        partial_value = jnp.dot(gated[:, lower:lower + group_width], out_weight[lower:lower + group_width], preferred_element_type=jnp.float32)
        mixed_sum = mixed_sum + lax.optimization_barrier(partial_value.astype(jnp.bfloat16)).astype(jnp.float32)
    residual = stream.astype(jnp.float32) + mixed_sum
    normed = (residual * lax.rsqrt(lax.optimization_barrier(jnp.mean(residual * residual, axis=-1, keepdims=True)) + EPSILON) * norm_gain.astype(jnp.float32)).astype(jnp.bfloat16)
    hidden_width = FF // N_TP
    feed_sum = jnp.zeros((length, D), jnp.float32)
    for group_index in range(N_TP):
        lower = group_index * hidden_width
        gate_pre = jnp.dot(normed, gate_weight[:, lower:lower + hidden_width], preferred_element_type=jnp.float32)
        up_value = jnp.dot(normed, up_weight[:, lower:lower + hidden_width], preferred_element_type=jnp.float32)
        hidden = (jax.nn.silu(gate_pre) * up_value).astype(jnp.bfloat16)
        partial_value = jnp.dot(hidden, down_weight[:, lower:lower + hidden_width].T, preferred_element_type=jnp.float32)
        feed_sum = feed_sum + lax.optimization_barrier(partial_value.astype(jnp.bfloat16)).astype(jnp.float32)
    return (residual + feed_sum).astype(jnp.bfloat16)
```

```python
import functools

import jax
import jax.numpy as jnp
from jax import lax
from jax.experimental import pallas as pl
from jax.experimental.pallas import tpu as pltpu
from jax.sharding import PartitionSpec as P

BLOCK = 128
FEATURE_BLOCK = 256
TILE = 256
HIGHEST = lax.Precision.HIGHEST
EPSILON = 1e-06
VERY_LOW = -1e30
MESH = pl.DeviceIdType.MESH


def two_pass(left, right, dims, split_left):
    wide = left if split_left else right
    high = wide.astype(jnp.bfloat16)
    low = (wide - high.astype(jnp.float32)).astype(jnp.bfloat16)
    total = None
    for part in (high, low):
        pair = (part, right) if split_left else (left, part)
        term = lax.dot_general(*pair, (dims, ((), ())), preferred_element_type=jnp.float32)
        total = term if total is None else total + term
    return total


def layer_kernel(
    n,
    heads,
    chunks,
    packed_ref,
    cols_ref,
    rows_ref,
    q_ref,
    k_ref,
    v_ref,
    og_ref,
    gain_ref,
    ng_ref,
    stream_ref,
    ow_ref,
    g_ref,
    u_ref,
    d_ref,
    out_ref,
    wgu,
    wd,
    ow_all,
    stream_all,
    gated_all,
    ng_all,
    normed,
    hidden,
    res,
    h_ref,
    c_ref,
    n_ref,
    m_ref,
    states,
    recv_a,
    recv_x,
    ring_s,
    ring_r,
    state_s,
    state_r,
    tp_s,
    tp_r,
    a_s,
    a_r,
    x_s,
    x_r,
    local_s,
):
    sp = lax.axis_index("sp")
    tp = lax.axis_index("tp")
    length = q_ref.shape[0]
    blocks = length // BLOCK
    units = 2 * heads
    depth_k = q_ref.shape[1] // heads
    depth_v = v_ref.shape[1] // heads
    wide_v = heads * depth_v
    width = stream_ref.shape[1]
    features = ow_ref.shape[1]
    shard, hw = d_ref.shape
    reach = n // 2

    near = tp + 1 - 2 * lax.rem(tp, 2)
    far = lax.rem(tp + 2, 4)
    cross = lax.rem(near + 2, 4)

    odd = lax.rem(sp, 2)
    pos = (1 - odd) * (sp // 2) + odd * (n - 1 - sp // 2)

    def at(place):
        place = lax.rem(place + 2 * n, n)
        second = place // (n // 2)
        return (1 - second) * 2 * place + second * (2 * (n - 1 - place) + 1)

    right, left = at(pos + 1), at(pos - 1)

    barrier = pltpu.get_barrier_semaphore()

    def greet(k, carry):
        pl.semaphore_signal(
            barrier, inc=1, device_id=(lax.rem(sp + k, n), tp), device_id_type=MESH
        )
        return carry

    lax.fori_loop(1, n, greet, 0)
    for other in (near, far):
        pl.semaphore_signal(barrier, inc=1, device_id=(sp, other), device_id_type=MESH)
    pl.semaphore_wait(barrier, n + 1)

    def state_copy(k):
        return pltpu.make_async_remote_copy(
            src_ref=packed_ref.at[(sp + k) // n],
            dst_ref=states.at[sp],
            send_sem=state_s.at[k],
            recv_sem=state_r.at[k],
            device_id=(lax.rem(sp + k, n), tp),
            device_id_type=MESH,
        )

    def state_arrival(k):
        slot = lax.rem(sp - k + n, n)
        return pltpu.make_async_remote_copy(
            src_ref=packed_ref.at[0],
            dst_ref=states.at[slot],
            send_sem=state_s.at[k],
            recv_sem=state_r.at[k],
            device_id=(slot, tp),
            device_id_type=MESH,
        )

    def send_state(k, carry):
        state_copy(k).start()
        return carry

    lax.fori_loop(1, n, send_state, 0)

    half = shard // 2

    def slot_view(kind, source):
        if kind == 0:
            return wgu.at[source, :, pl.ds(0, hw)]
        if kind == 1:
            return wgu.at[source, :, pl.ds(hw, hw)]
        return wd.at[source, pl.ds((kind - 2) * half, half), :]

    def own_view(kind):
        if kind == 0:
            return g_ref
        if kind == 1:
            return u_ref
        return d_ref.at[pl.ds((kind - 2) * half, half), :]

    def ring_copy(way, kind, step):
        source = at(pos - step) if way == 0 else at(pos + step)
        return pltpu.make_async_remote_copy(
            src_ref=own_view(kind) if step == 0 else slot_view(kind, source),
            dst_ref=slot_view(kind, source),
            send_sem=ring_s.at[way, kind, step],
            recv_sem=ring_r.at[way, kind, step],
            device_id=(right if way == 0 else left, tp),
            device_id_type=MESH,
        )

    def ring_arrival(way, kind, step):
        source = at(pos - step - 1) if way == 0 else at(pos + step + 1)
        view = slot_view(kind, source)
        return pltpu.make_async_remote_copy(
            src_ref=view,
            dst_ref=view,
            send_sem=ring_s.at[way, kind, step],
            recv_sem=ring_r.at[way, kind, step],
            device_id=(right if way == 0 else left, tp),
            device_id_type=MESH,
        )

    def kind_of(way, base, turn):
        return base + (turn if way == 0 else 1 - turn)

    def launch(base):
        for turn in range(2):
            for way in range(2):
                ring_copy(way, kind_of(way, base, turn), 0).start()

    def arrive(base, turn, step):
        for way in range(2):
            ring_arrival(way, kind_of(way, base, turn), step).wait_recv()

    def advance(event):
        base, turn, step = event
        for way in range(2):
            kind = kind_of(way, base, turn)
            ring_arrival(way, kind, step - 1).wait_recv()
            ring_copy(way, kind, step).start()

    def events(base):
        return [(base, turn, step) for step in range(1, reach) for turn in range(2)][:-1]

    gu_events = events(0)
    d_events = events(2)
    launch(0)

    chunk = length // chunks
    items = [("ow", 0), ("ng", 0)]
    items += [("stream", i) for i in range(chunks)]
    items += [("gated", i) for i in range(chunks)]

    def tp_view(item, slot):
        what, i = item
        if what == "ow":
            return ow_all.at[pl.ds(pl.multiple_of(slot * wide_v, wide_v), wide_v), :]
        if what == "ng":
            return ng_all.at[:, pl.ds(pl.multiple_of(slot * width, width), width)]
        if what == "stream":
            return stream_all.at[
                pl.ds(i * chunk, chunk), pl.ds(pl.multiple_of(slot * width, width), width)
            ]
        return gated_all.at[
            pl.ds(i * chunk, chunk), pl.ds(pl.multiple_of(slot * wide_v, wide_v), wide_v)
        ]

    def tp_own(item):
        what, i = item
        if what == "ow":
            return ow_ref
        if what == "ng":
            return ng_ref
        if what == "stream":
            return stream_ref.at[pl.ds(i * chunk, chunk), :]
        return tp_view(item, tp)

    def tp_copy(item, route):
        number = items.index(item)
        slot = tp if route < 2 else far
        return pltpu.make_async_remote_copy(
            src_ref=tp_own(item) if route < 2 else tp_view(item, far),
            dst_ref=tp_view(item, slot),
            send_sem=tp_s.at[route, number],
            recv_sem=tp_r.at[route, number],
            device_id=(sp, far if route == 0 else near),
            device_id_type=MESH,
        )

    def tp_arrival(item, route):
        number = items.index(item)
        view = tp_view(item, (far, near, cross)[route])
        return pltpu.make_async_remote_copy(
            src_ref=view,
            dst_ref=view,
            send_sem=tp_s.at[route, number],
            recv_sem=tp_r.at[route, number],
            device_id=(sp, far if route == 0 else near),
            device_id_type=MESH,
        )

    def share(item):
        for route in range(2):
            tp_copy(item, route).start()

    def relay(item):
        tp_arrival(item, 0).wait_recv()
        tp_copy(item, 2).start()

    def settle(item):
        for route in (1, 2):
            tp_arrival(item, route).wait_recv()

    early = items[: 2 + chunks]
    late = items[2 + chunks :]
    for item in early:
        share(item)

    own = [
        pltpu.make_async_copy(g_ref, slot_view(0, sp), local_s.at[0]),
        pltpu.make_async_copy(u_ref, slot_view(1, sp), local_s.at[1]),
        pltpu.make_async_copy(d_ref, wd.at[sp], local_s.at[2]),
        pltpu.make_async_copy(ow_ref, tp_view(("ow", 0), tp), local_s.at[3]),
        pltpu.make_async_copy(
            stream_ref,
            stream_all.at[:, pl.ds(pl.multiple_of(tp * width, width), width)],
            local_s.at[4],
        ),
        pltpu.make_async_copy(ng_ref, tp_view(("ng", 0), tp), local_s.at[5]),
    ]
    for copy in own:
        copy.start()

    def wait_state(k, carry):
        state_arrival(k).wait_recv()
        return carry

    lax.fori_loop(1, n, wait_state, 0)
    for direction in range(2):
        for head in range(heads):
            unit = direction * heads + head

            def take(j, carry):
                matrix, normer, peak = carry
                item = states[j if direction == 0 else n - 1 - j, head]
                their_peak = item[depth_k + 1 : depth_k + 2]
                decayed = peak + item[depth_k + 2 : depth_k + 3]
                new_peak = jnp.maximum(decayed, their_peak)
                keep = jnp.exp(decayed - new_peak)
                gain = jnp.exp(their_peak - new_peak)
                return (
                    keep * matrix + gain * item[:depth_k],
                    keep * normer + gain * item[depth_k : depth_k + 1],
                    new_peak,
                )

            zero = jnp.zeros((1, BLOCK), jnp.float32)
            matrix, normer, peak = lax.fori_loop(
                0,
                sp if direction == 0 else n - 1 - sp,
                take,
                (jnp.zeros((depth_k, depth_v), jnp.float32), zero, zero),
            )
            c_ref[unit] = jnp.zeros(c_ref.shape[1:], jnp.float32)
            c_ref[unit, head * depth_k : (head + 1) * depth_k, :] = matrix
            n_ref[unit] = normer
            m_ref[unit] = peak

    at_row = lax.broadcasted_iota(jnp.int32, (BLOCK, BLOCK), 0)
    at_col = lax.broadcasted_iota(jnp.int32, (BLOCK, BLOCK), 1)
    lane = lax.broadcasted_iota(jnp.int32, (BLOCK, q_ref.shape[1]), 1)

    def step(index, carry):
        for direction in range(2):
            block = index if direction == 0 else blocks - 1 - index
            rows = pl.ds(pl.multiple_of(block * BLOCK, BLOCK), BLOCK)
            query = q_ref[rows, :].astype(jnp.float32) * depth_k ** (-0.5)
            key = k_ref[rows, :]
            key_wide = key.astype(jnp.float32)
            cols = cols_ref[rows, :]
            row_block = rows_ref[block]
            keep = at_col <= at_row if direction == 0 else at_col >= at_row
            for head in range(heads):
                unit = direction * heads + head
                mine = (lane >= head * depth_k) & (lane < (head + 1) * depth_k)
                q_wide = jnp.where(mine, query, 0.0)
                q_own = q_wide.astype(jnp.bfloat16)
                value = v_ref[rows, head * depth_v : (head + 1) * depth_v]
                b_col = cols[:, unit : unit + 1]
                a_col = cols[:, units + unit : units + unit + 1]
                a_row = row_block[unit : unit + 1, :]
                total = row_block[units + unit : units + unit + 1, :]
                m_row = m_ref[unit]
                n_row = n_ref[unit]
                c_state = c_ref[unit]
                decay = jnp.where(keep, b_col + a_row, VERY_LOW)
                carry_log = b_col + m_row[:, :1]
                peak = jnp.maximum(carry_log, jnp.max(decay, axis=1, keepdims=True))
                scores = lax.dot_general(
                    q_own, key, (((1,), (1,)), ((), ())), preferred_element_type=jnp.float32
                ) * jnp.exp(decay - peak)
                carried = jnp.exp(carry_log - peak)
                number = two_pass(scores, value, ((1,), (0,)), True)
                number = number + carried * two_pass(q_own, c_state, ((1,), (0,)), False)
                below = jnp.sum(scores, axis=1, keepdims=True)
                below = below + carried * jnp.sum(q_wide * n_row, axis=1, keepdims=True)
                h_ref[direction, rows, head * depth_v : (head + 1) * depth_v] = number / jnp.maximum(
                    jnp.abs(below), jnp.exp(-peak)
                )
                new_m = jnp.maximum(total + m_row, total + jnp.max(a_row, axis=1, keepdims=True))
                shrink = jnp.exp(total + m_row - new_m)
                weight = jnp.exp(total[:, :1] + a_col - new_m[:, :1])
                weighted = weight * value.astype(jnp.float32)
                c_ref[unit] = shrink[:, :1] * c_state + two_pass(
                    key, weighted, ((0,), (0,)), False
                )
                n_ref[unit] = shrink[:, :1] * n_row + jnp.sum(
                    weight * key_wide, axis=0, keepdims=True
                )
                m_ref[unit] = new_m

        @pl.when(index == (2 * blocks) // 3)
        def _():
            advance(gu_events[0])

        return carry

    lax.fori_loop(0, blocks, step, 0)

    def finish(index, carry):
        rows = pl.ds(pl.multiple_of(index * BLOCK, BLOCK), BLOCK)
        for head in range(heads):
            span = slice(head * depth_v, (head + 1) * depth_v)
            summed = h_ref[0, rows, span] + h_ref[1, rows, span]
            scale = lax.rsqrt(jnp.mean(summed * summed, axis=1, keepdims=True) + EPSILON)
            opened = 1.0 / (1.0 + jnp.exp(-og_ref[rows, span].astype(jnp.float32)))
            place = pl.multiple_of(tp * wide_v + head * depth_v, depth_v)
            gated_all[rows, pl.ds(place, depth_v)] = (
                summed * scale * gain_ref[:, span] * opened
            ).astype(jnp.bfloat16)
        return carry

    lax.fori_loop(0, blocks, finish, 0)
    for item in late:
        share(item)

    advance(gu_events[1])
    relay(("ow", 0))
    relay(("ng", 0))
    relay(early[2])
    relay(early[3])
    advance(gu_events[2])
    for item in early[4:]:
        relay(item)
    relay(late[0])
    advance(gu_events[3])
    for item in late[1:]:
        relay(item)
    for item in items:
        settle(item)
    for copy in own:
        copy.wait()

    def project(index, carry):
        rows = pl.ds(pl.multiple_of(index * TILE, TILE), TILE)
        total = stream_all[rows, :].astype(jnp.float32) + jnp.dot(
            gated_all[rows, :], ow_all[...], preferred_element_type=jnp.float32
        )
        scale = lax.rsqrt(jnp.mean(total * total, axis=1, keepdims=True) + EPSILON)
        normed[rows, :] = (total * scale * ng_all[0:1, :]).astype(jnp.bfloat16)
        for j in range(features // width):

            @pl.when(tp == j)
            def _():
                res[rows, :] = total[:, j * width : (j + 1) * width]

        @pl.when(index == 2)
        def _():
            advance(gu_events[4])

        return carry

    lax.fori_loop(0, length // TILE, project, 0)
    for event in gu_events[5:]:
        advance(event)
    launch(2)
    if reach >= 2:
        arrive(0, 1, reach - 2)
    arrive(0, 0, reach - 1)

    slab = 256
    part_rows = length // 2

    def activate(gate, up):
        return (gate / (1.0 + jnp.exp(-gate)) * up).astype(jnp.bfloat16)

    def open_slab(index, carry):
        first = pl.multiple_of(index * slab, slab)
        gate_cut = wgu[:, :, pl.ds(first, slab)].reshape(features, slab)
        up_cut = wgu[:, :, pl.ds(pl.multiple_of(hw + index * slab, BLOCK), slab)].reshape(
            features, slab
        )
        for part in range(2):
            rows = slice(part * part_rows, (part + 1) * part_rows)
            gate = jnp.dot(normed[rows, :], gate_cut, preferred_element_type=jnp.float32)
            up = jnp.dot(normed[rows, :], up_cut, preferred_element_type=jnp.float32)
            hidden[rows, pl.ds(first, slab)] = activate(gate, up)
        for at_slab, number in ((2, 0), (4, 1)):

            @pl.when(index == at_slab)
            def _():
                advance(d_events[number])

        return carry

    slabs = hw // slab
    lax.fori_loop(0, slabs, open_slab, 0)
    rest = hw - slabs * slab
    if rest:
        cut = jnp.concatenate(
            [wgu[:, :, slabs * slab : hw], wgu[:, :, hw + slabs * slab :]], axis=2
        ).reshape(features, 2 * rest)
        for part in range(2):
            rows = slice(part * part_rows, (part + 1) * part_rows)
            both = jnp.dot(normed[rows, :], cut, preferred_element_type=jnp.float32)
            hidden[rows, slabs * slab :] = activate(both[:, :rest], both[:, rest:])

    per_owner = width // FEATURE_BLOCK
    group = FEATURE_BLOCK // shard

    def stage(slot):
        return normed.at[:, pl.ds(pl.multiple_of(slot * FEATURE_BLOCK, FEATURE_BLOCK), FEATURE_BLOCK)]

    def a_copy(slot):
        return pltpu.make_async_remote_copy(
            src_ref=stage(slot),
            dst_ref=recv_a.at[slot],
            send_sem=a_s.at[slot],
            recv_sem=a_r.at[slot],
            device_id=(sp, near),
            device_id_type=MESH,
        )

    def x_copy(slot):
        return pltpu.make_async_remote_copy(
            src_ref=stage(2 * per_owner + slot),
            dst_ref=recv_x.at[slot],
            send_sem=x_s.at[slot],
            recv_sem=x_r.at[slot],
            device_id=(sp, far),
            device_id_type=MESH,
        )

    if group > 1:
        for event in d_events[2:]:
            advance(event)
        arrive(2, 1, reach - 2)
        arrive(2, 0, reach - 1)

    def lower(index, carry):
        if group == 1:
            hop = (index + 1) // 2
            block = at(pos + hop * (1 - 2 * lax.rem(index, 2)))
            for number, event in enumerate(d_events[2:]):

                @pl.when(index == 2 * event[2] - 1)
                def _():
                    advance(event)

            @pl.when(index == 2 * reach - 3)
            def _():
                arrive(2, 1, reach - 2)

            @pl.when(index == 2 * reach - 1)
            def _():
                arrive(2, 0, reach - 1)

            cut = wd[block]
        else:
            block = index
            cut = wd[pl.ds(pl.multiple_of(block * group, group), group)].reshape(FEATURE_BLOCK, hw)
        owner = block // per_owner
        slot = lax.rem(block, per_owner)
        low = lax.rem(lax.rem(tp, 2) + lax.rem(owner, 2), 2)
        high = lax.rem(tp // 2 + owner // 2, 2)
        part = lax.dot_general(
            hidden[...], cut, (((1,), (1,)), ((), ())), preferred_element_type=jnp.float32
        )

        @pl.when(low == 1)
        def _():
            place = high * per_owner + slot
            first = pl.multiple_of(place * FEATURE_BLOCK, FEATURE_BLOCK)
            normed[:, pl.ds(first, FEATURE_BLOCK)] = part.astype(jnp.bfloat16)
            a_copy(place).start()

        @pl.when((low == 0) & (high == 0))
        def _():
            first = pl.multiple_of(slot * FEATURE_BLOCK, FEATURE_BLOCK)
            res[:, pl.ds(first, FEATURE_BLOCK)] = res[:, pl.ds(first, FEATURE_BLOCK)] + part

        @pl.when((low == 0) & (high == 1))
        def _():
            a_copy(per_owner + slot).wait_recv()
            first = pl.multiple_of((2 * per_owner + slot) * FEATURE_BLOCK, FEATURE_BLOCK)
            normed[:, pl.ds(first, FEATURE_BLOCK)] = (
                part + recv_a[per_owner + slot].astype(jnp.float32)
            ).astype(jnp.bfloat16)
            x_copy(slot).start()

        return carry

    lax.fori_loop(0, features // FEATURE_BLOCK, lower, 0)

    for slot in range(per_owner):
        a_copy(slot).wait_recv()
        x_copy(slot).wait_recv()
        span = slice(slot * FEATURE_BLOCK, (slot + 1) * FEATURE_BLOCK)
        out_ref[:, span] = (
            res[:, span] + recv_a[slot].astype(jnp.float32) + recv_x[slot].astype(jnp.float32)
        ).astype(jnp.bfloat16)

    def state_left(k, carry):
        state_copy(k).wait_send()
        return carry

    lax.fori_loop(1, n, state_left, 0)
    for base in (0, 2):
        for way in range(2):
            for turn in range(2):
                ring_copy(way, kind_of(way, base, turn), 0).wait_send()
        for _, turn, hop in events(base):
            for way in range(2):
                ring_copy(way, kind_of(way, base, turn), hop).wait_send()
    for item in items:
        for route in range(3):
            tp_copy(item, route).wait_send()
    for slot in range(2 * per_owner):
        a_copy(slot).wait_send()
    for slot in range(per_owner):
        x_copy(slot).wait_send()


def local(
    query,
    key_rows,
    value,
    in_gate,
    forget_pre,
    out_gate,
    head_gain,
    out_weight,
    stream,
    norm_gain,
    gate_weight,
    up_weight,
    down_weight,
):
    length = query.shape[0]
    heads = in_gate.shape[1]
    depth_k = query.shape[1] // heads
    depth_v = value.shape[1] // heads
    blocks = length // BLOCK
    n_sp = lax.axis_size("sp")
    n_tp = lax.axis_size("tp")
    assert n_tp == 4 and n_sp % 2 == 0
    width = stream.shape[1]
    features = width * n_tp
    shard, hidden_width = gate_weight.shape
    units = 2 * heads

    forgets = jax.nn.log_sigmoid(forget_pre).reshape(2, heads, blocks, BLOCK)
    gates = in_gate.reshape(2, heads, blocks, BLOCK)
    upper = jnp.triu(jnp.ones((BLOCK, BLOCK), jnp.float32))
    tri = jnp.stack([upper, upper.T])
    b = jnp.einsum("dhns,dsj->dhnj", forgets, tri, precision=HIGHEST)
    a = gates - b
    total = jnp.sum(forgets, axis=-1)
    grid_n = jnp.arange(blocks)
    later = (grid_n[:, None] < grid_n[None, :]).astype(jnp.float32)
    following = jnp.stack(
        [
            jnp.sum(total[0][:, None, :] * later[None], axis=-1),
            jnp.sum(total[1][:, None, :] * later.T[None], axis=-1),
        ]
    )
    own_log = (total + following)[..., None] + a
    own_peak = jnp.max(own_log, axis=(2, 3))
    own_total = jnp.sum(total, axis=-1)
    own_weight = jnp.exp(own_log - own_peak[..., None, None]).reshape(units, length)
    key_wide = key_rows.astype(jnp.float32)
    matrices = []
    for unit in range(units):
        head = unit % heads
        weighted = own_weight[unit][:, None] * value[:, head * depth_v : (head + 1) * depth_v].astype(
            jnp.float32
        )
        matrices.append(
            lax.dot_general(
                key_rows,
                weighted.astype(jnp.bfloat16),
                (((0,), (0,)), ((), ())),
                preferred_element_type=jnp.float32,
            )[head * depth_k : (head + 1) * depth_k]
        )
    matrix = jnp.stack(matrices)
    normer_all = jnp.dot(own_weight, key_wide, precision=HIGHEST)
    of_head = jnp.arange(heads * depth_k)[None, :] // depth_k == (jnp.arange(units) % heads)[:, None]
    normer = jnp.where(of_head, normer_all, 0.0)
    normer = jnp.pad(normer, ((0, 0), (0, depth_v - heads * depth_k)))
    packed = jnp.concatenate(
        [
            matrix,
            normer[:, None, :],
            jnp.broadcast_to(own_peak.reshape(units, 1, 1), (units, 1, depth_v)),
            jnp.broadcast_to(own_total.reshape(units, 1, 1), (units, 1, depth_v)),
            jnp.zeros((units, 5, depth_v), jnp.float32),
        ],
        axis=1,
    ).reshape(2, heads, depth_k + 8, depth_v)
    cols = jnp.concatenate([b.reshape(units, length), a.reshape(units, length)], axis=0).T
    rows = jnp.concatenate(
        [
            a.reshape(units, blocks, BLOCK),
            jnp.broadcast_to(total.reshape(units, blocks, 1), (units, blocks, BLOCK)),
        ],
        axis=0,
    ).transpose(1, 0, 2)
    chunks = next(c for c in (3, 2, 1) if blocks % c == 0)
    per_owner = width // FEATURE_BLOCK
    reach = n_sp // 2
    wide_v = heads * depth_v
    dma = pltpu.SemaphoreType.DMA
    bf16, f32 = jnp.bfloat16, jnp.float32
    vmem = pl.BlockSpec(memory_space=pltpu.VMEM)
    anywhere = pl.BlockSpec(memory_space=pl.ANY)
    return pl.pallas_call(
        functools.partial(layer_kernel, n_sp, heads, chunks),
        out_shape=jax.ShapeDtypeStruct((length, width), bf16),
        in_specs=[vmem] * 9 + [anywhere] * 5,
        out_specs=vmem,
        scratch_shapes=[
            pltpu.VMEM((n_sp, shard, 2 * hidden_width), bf16),
            pltpu.VMEM((n_sp, shard, hidden_width), bf16),
            pltpu.VMEM((n_tp * wide_v, features), bf16),
            pltpu.VMEM((length, features), bf16),
            pltpu.VMEM((length, n_tp * wide_v), bf16),
            pltpu.VMEM((8, features), f32),
            pltpu.VMEM((length, features), bf16),
            pltpu.VMEM((length, hidden_width), bf16),
            pltpu.VMEM((length, width), f32),
            pltpu.VMEM((2, length, wide_v), f32),
            pltpu.VMEM((units, heads * depth_k, depth_v), f32),
            pltpu.VMEM((units, 1, heads * depth_k), f32),
            pltpu.VMEM((units, 1, BLOCK), f32),
            pltpu.VMEM((n_sp, heads, depth_k + 8, depth_v), f32),
            pltpu.VMEM((2 * per_owner, length, FEATURE_BLOCK), bf16),
            pltpu.VMEM((per_owner, length, FEATURE_BLOCK), bf16),
            dma((2, 4, reach)),
            dma((2, 4, reach)),
            dma((n_sp,)),
            dma((n_sp,)),
            dma((3, 2 + 2 * chunks)),
            dma((3, 2 + 2 * chunks)),
            dma((2 * per_owner,)),
            dma((2 * per_owner,)),
            dma((per_owner,)),
            dma((per_owner,)),
            dma((6,)),
        ],
        compiler_params=pltpu.CompilerParams(
            collective_id=0, has_side_effects=True, vmem_limit_bytes=67_000_000
        ),
        name="layer",
    )(
        packed,
        cols,
        rows,
        query,
        key_rows,
        value,
        out_gate,
        head_gain.astype(f32)[None, :],
        jnp.broadcast_to(norm_gain.astype(f32)[None, :], (8, width)),
        stream,
        out_weight,
        gate_weight,
        up_weight,
        down_weight,
    )


def solution(mesh):
    placed = (
        P("sp", "tp"),
        P("sp", "tp"),
        P("sp", "tp"),
        P(None, "tp", "sp"),
        P(None, "tp", "sp"),
        P("sp", "tp"),
        P("tp"),
        P("tp", None),
        P("sp", "tp"),
        P("tp"),
        P("sp", "tp"),
        P("sp", "tp"),
        P("sp", "tp"),
    )
    return jax.shard_map(
        local, mesh=mesh, in_specs=placed, out_specs=P("sp", "tp"), check_vma=False
    )
```

```python
import functools

import jax
import jax.numpy as jnp
from jax import lax
from jax.experimental import pallas as pl
from jax.experimental.pallas import tpu as pltpu
from jax.sharding import PartitionSpec as P

BLOCK = 128
PIECE = 128
TILE = 256
HIGHEST = lax.Precision.HIGHEST
EPSILON = 1e-06
VERY_LOW = -1e30
MESH = pl.DeviceIdType.MESH


def two_pass(left, right, dims, split_left):
    wide = left if split_left else right
    high = wide.astype(jnp.bfloat16)
    low = (wide - high.astype(jnp.float32)).astype(jnp.bfloat16)
    total = None
    for part in (high, low):
        pair = (part, right) if split_left else (left, part)
        term = lax.dot_general(*pair, (dims, ((), ())), preferred_element_type=jnp.float32)
        total = term if total is None else total + term
    return total


def layer_kernel(
    n,
    heads,
    chunks,
    gate_in,
    forget_in,
    gain_ref,
    q_in,
    k_in,
    v_in,
    og_in,
    ng_ref,
    stream_ref,
    ow_ref,
    g_ref,
    u_ref,
    d_ref,
    out_ref,
    q_ref,
    k_ref,
    v_ref,
    og_ref,
    a_ref,
    b_ref,
    w_ref,
    total_ref,
    cols_ref,
    both,
    pair_sum,
    wgu,
    wd,
    ow_all,
    stream_all,
    gated_all,
    ng_all,
    normed,
    hidden,
    res,
    h_ref,
    c_ref,
    n_ref,
    m_ref,
    others,
    recv_a,
    recv_x,
    ring_s,
    ring_r,
    mate_s,
    mate_r,
    state_s,
    state_r,
    tp_s,
    tp_r,
    a_s,
    a_r,
    x_s,
    x_r,
    local_s,
):
    sp = lax.axis_index("sp")
    tp = lax.axis_index("tp")
    length = q_ref.shape[0]
    blocks = length // BLOCK
    units = 2 * heads
    depth_k = q_ref.shape[1] // heads
    depth_v = v_ref.shape[1] // heads
    wide_v = heads * depth_v
    width = stream_ref.shape[1]
    features = ow_ref.shape[1]
    shard, hw = d_ref.shape
    reach = n // 2

    near = tp + 1 - 2 * lax.rem(tp, 2)
    far = lax.rem(tp + 2, 4)
    cross = lax.rem(near + 2, 4)

    odd = lax.rem(sp, 2)
    pos = (1 - odd) * (sp // 2) + odd * (n - 1 - sp // 2)

    def at(place):
        place = lax.rem(place + 2 * n, n)
        second = place // (n // 2)
        return (1 - second) * 2 * place + second * (2 * (n - 1 - place) + 1)

    right, left = at(pos + 1), at(pos - 1)
    pairs = n // 2
    pair, member = sp // 2, lax.rem(sp, 2)
    mate = sp + 1 - 2 * member

    inputs = [
        pltpu.make_async_copy(source, target, local_s.at[6 + i])
        for i, (source, target) in enumerate(
            ((k_in, k_ref), (v_in, v_ref), (q_in, q_ref), (og_in, og_ref))
        )
    ]
    for copy in inputs:
        copy.start()

    barrier = pltpu.get_barrier_semaphore()

    def greet(k, carry):
        pl.semaphore_signal(
            barrier, inc=1, device_id=(lax.rem(sp + k, n), tp), device_id_type=MESH
        )
        return carry

    lax.fori_loop(1, n, greet, 0)
    for other in (near, far):
        pl.semaphore_signal(barrier, inc=1, device_id=(sp, other), device_id_type=MESH)
    pl.semaphore_wait(barrier, n + 1)

    half = shard // 2

    def slot_view(kind, source):
        if kind == 0:
            return wgu.at[source, :, pl.ds(0, hw)]
        if kind == 1:
            return wgu.at[source, :, pl.ds(hw, hw)]
        return wd.at[source, pl.ds((kind - 2) * half, half), :]

    def own_view(kind):
        if kind == 0:
            return g_ref
        if kind == 1:
            return u_ref
        return d_ref.at[pl.ds((kind - 2) * half, half), :]

    def ring_copy(way, kind, step):
        source = at(pos - step) if way == 0 else at(pos + step)
        return pltpu.make_async_remote_copy(
            src_ref=own_view(kind) if step == 0 else slot_view(kind, source),
            dst_ref=slot_view(kind, source),
            send_sem=ring_s.at[way, kind, step],
            recv_sem=ring_r.at[way, kind, step],
            device_id=(right if way == 0 else left, tp),
            device_id_type=MESH,
        )

    def ring_arrival(way, kind, step):
        source = at(pos - step - 1) if way == 0 else at(pos + step + 1)
        view = slot_view(kind, source)
        return pltpu.make_async_remote_copy(
            src_ref=view,
            dst_ref=view,
            send_sem=ring_s.at[way, kind, step],
            recv_sem=ring_r.at[way, kind, step],
            device_id=(right if way == 0 else left, tp),
            device_id_type=MESH,
        )

    def launch(base, turn):
        for way in range(2):
            ring_copy(way, kind_of(way, base, turn), 0).start()

    def launch_part(first, size):
        for way in range(2):
            rows = pl.ds(first, size)
            pltpu.make_async_remote_copy(
                src_ref=own_view(way).at[rows, :],
                dst_ref=wgu.at[sp, rows, pl.ds(way * hw, hw)],
                send_sem=ring_s.at[way, way, 0],
                recv_sem=ring_r.at[way, way, 0],
                device_id=(right if way == 0 else left, tp),
                device_id_type=MESH,
            ).start()

    quarter = shard // 4

    def kind_of(way, base, turn):
        return base + (turn if way == 0 else 1 - turn)

    def arrive(base, turn, step):
        for way in range(2):
            ring_arrival(way, kind_of(way, base, turn), step).wait_recv()

    def advance(event):
        base, turn, step = event
        for way in range(2):
            kind = kind_of(way, base, turn)
            ring_arrival(way, kind, step - 1).wait_recv()
            ring_copy(way, kind, step).start()

    def events(base):
        return [(base, turn, step) for step in range(1, reach) for turn in range(2)][:-1]

    gu_events = events(0)
    d_events = events(2)
    launch_part(0, quarter)

    chunk = length // chunks
    items = [("ow", 0), ("ng", 0)]
    items += [("stream", i) for i in range(chunks)]
    items += [("gated", i) for i in range(chunks)]

    def tp_view(item, slot):
        what, i = item
        if what == "ow":
            return ow_all.at[pl.ds(pl.multiple_of(slot * wide_v, wide_v), wide_v), :]
        if what == "ng":
            return ng_all.at[pl.ds(pl.multiple_of(slot * width, width), width)]
        if what == "stream":
            return stream_all.at[
                pl.ds(i * chunk, chunk), pl.ds(pl.multiple_of(slot * width, width), width)
            ]
        return gated_all.at[
            pl.ds(i * chunk, chunk), pl.ds(pl.multiple_of(slot * wide_v, wide_v), wide_v)
        ]

    def tp_own(item):
        what, i = item
        if what == "ow":
            return ow_ref
        if what == "ng":
            return ng_ref
        if what == "stream":
            return stream_ref.at[pl.ds(i * chunk, chunk), :]
        return tp_view(item, tp)

    def tp_copy(item, route):
        number = items.index(item)
        slot = tp if route < 2 else far
        return pltpu.make_async_remote_copy(
            src_ref=tp_own(item) if route < 2 else tp_view(item, far),
            dst_ref=tp_view(item, slot),
            send_sem=tp_s.at[route, number],
            recv_sem=tp_r.at[route, number],
            device_id=(sp, far if route == 0 else near),
            device_id_type=MESH,
        )

    def tp_arrival(item, route):
        number = items.index(item)
        view = tp_view(item, (far, near, cross)[route])
        return pltpu.make_async_remote_copy(
            src_ref=view,
            dst_ref=view,
            send_sem=tp_s.at[route, number],
            recv_sem=tp_r.at[route, number],
            device_id=(sp, far if route == 0 else near),
            device_id_type=MESH,
        )

    def share(item):
        for route in range(2):
            tp_copy(item, route).start()

    def relay(item):
        tp_arrival(item, 0).wait_recv()
        tp_copy(item, 2).start()

    def settle(item):
        for route in (1, 2):
            tp_arrival(item, route).wait_recv()

    early = items[: 2 + chunks]
    late = items[2 + chunks :]
    for item in early:
        share(item)

    own = [
        pltpu.make_async_copy(g_ref, slot_view(0, sp), local_s.at[0]),
        pltpu.make_async_copy(u_ref, slot_view(1, sp), local_s.at[1]),
        pltpu.make_async_copy(d_ref, wd.at[sp], local_s.at[2]),
        pltpu.make_async_copy(ow_ref, tp_view(("ow", 0), tp), local_s.at[3]),
        pltpu.make_async_copy(
            stream_ref,
            stream_all.at[:, pl.ds(pl.multiple_of(tp * width, width), width)],
            local_s.at[4],
        ),
        pltpu.make_async_copy(ng_ref, tp_view(("ng", 0), tp), local_s.at[5]),
    ]
    for copy in own:
        copy.start()

    both[member] = jnp.zeros(both.shape[1:], jnp.float32)

    for copy in inputs:
        copy.wait()
    for block in range(blocks):
        for unit in range(units):
            spot = block * units + unit
            tokens = slice(block * BLOCK, (block + 1) * BLOCK)
            a_ref[spot : spot + 1, :] = gate_in[unit // heads, unit % heads : unit % heads + 1, tokens]
            b_ref[spot : spot + 1, :] = forget_in[
                unit // heads, unit % heads : unit % heads + 1, tokens
            ]
    raw = b_ref[...]
    forgets = jnp.minimum(raw, 0.0) - jnp.log1p(jnp.exp(-jnp.abs(raw)))
    at_row = lax.broadcasted_iota(jnp.int32, (BLOCK, BLOCK), 0)
    at_col = lax.broadcasted_iota(jnp.int32, (BLOCK, BLOCK), 1)
    upto = (at_row <= at_col).astype(jnp.bfloat16)
    since = (at_row >= at_col).astype(jnp.bfloat16)
    first = forgets.astype(jnp.bfloat16)
    left_over = forgets - first.astype(jnp.float32)
    second = left_over.astype(jnp.bfloat16)
    third = (left_over - second.astype(jnp.float32)).astype(jnp.bfloat16)
    ahead = jnp.zeros_like(forgets)
    behind = jnp.zeros_like(forgets)
    for piece in (third, second, first):
        ahead = ahead + jnp.dot(piece, upto, preferred_element_type=jnp.float32)
        behind = behind + jnp.dot(piece, since, preferred_element_type=jnp.float32)
    spots = lax.broadcasted_iota(jnp.int32, forgets.shape, 0)
    sums = jnp.where(lax.rem(spots, units) < heads, ahead, behind)
    shifted = a_ref[...] - sums
    b_ref[...] = sums
    a_ref[...] = shifted
    total_ref[...] = jnp.broadcast_to(jnp.sum(forgets, axis=1, keepdims=True), forgets.shape)
    peaks = []
    for unit in range(units):
        direction = unit // heads
        beyond = jnp.zeros((1, BLOCK), jnp.float32)
        order = range(blocks - 1, -1, -1) if direction == 0 else range(blocks)
        highest = None
        for block in order:
            spot = block * units + unit
            beyond = beyond + total_ref[spot : spot + 1, :]
            logs = beyond + a_ref[spot : spot + 1, :]
            w_ref[spot : spot + 1, :] = logs
            highest = logs if highest is None else jnp.maximum(highest, logs)
        highest = jnp.broadcast_to(jnp.max(highest, axis=1, keepdims=True), (1, BLOCK))
        peaks.append(highest)
        head = unit % heads
        both[member, direction, head, depth_k + 1 : depth_k + 2, :] = highest
        both[member, direction, head, depth_k + 2 : depth_k + 3, :] = beyond
    for block in range(blocks):
        spot = slice(block * units, (block + 1) * units)
        w_ref[spot, :] = jnp.exp(w_ref[spot, :] - jnp.concatenate(peaks, axis=0))

    lane = lax.broadcasted_iota(jnp.int32, (BLOCK, q_ref.shape[1]), 1)
    lane_row = lax.broadcasted_iota(jnp.int32, (1, q_ref.shape[1]), 1)

    def turn_block(block, normers):
        rows = pl.ds(pl.multiple_of(block * BLOCK, BLOCK), BLOCK)
        spot = pl.ds(block * units, units)
        stacked = jnp.concatenate([b_ref[spot, :], a_ref[spot, :], w_ref[spot, :], w_ref[spot, :]], axis=0)
        columns = stacked.T
        cols_ref[rows, : 4 * units] = columns
        key_wide = k_ref[rows, :].astype(jnp.float32)
        out = []
        for unit in range(units):
            head = unit % heads
            weight = columns[:, 2 * units + unit : 2 * units + unit + 1]
            value = v_ref[rows, head * depth_v : (head + 1) * depth_v].astype(jnp.float32)
            hidden[rows, unit * depth_v : (unit + 1) * depth_v] = (weight * value).astype(jnp.bfloat16)
            out.append(normers[unit] + jnp.sum(weight * key_wide, axis=0, keepdims=True))
        return tuple(out)

    normers = lax.fori_loop(
        0,
        blocks,
        turn_block,
        tuple(jnp.zeros((1, heads * depth_k), jnp.float32) for _ in range(units)),
    )
    outer = lax.dot_general(
        k_ref[...],
        hidden[:, : units * depth_v],
        (((0,), (0,)), ((), ())),
        preferred_element_type=jnp.float32,
    )
    for unit in range(units):
        direction, head = unit // heads, unit % heads
        both[member, direction, head, :depth_k, :] = outer[
            head * depth_k : (head + 1) * depth_k, unit * depth_v : (unit + 1) * depth_v
        ]
        mine = (lane_row >= head * depth_k) & (lane_row < (head + 1) * depth_k)
        both[member, direction, head, depth_k : depth_k + 1, :] = jnp.where(mine, normers[unit], 0.0)

    def mate_copy(which):
        return pltpu.make_async_remote_copy(
            src_ref=both.at[which],
            dst_ref=both.at[which],
            send_sem=mate_s,
            recv_sem=mate_r,
            device_id=(mate, tp),
            device_id_type=MESH,
        )

    def state_copy(k):
        return pltpu.make_async_remote_copy(
            src_ref=pair_sum.at[(pair + k) // pairs],
            dst_ref=others.at[pair],
            send_sem=state_s.at[k],
            recv_sem=state_r.at[k],
            device_id=(2 * lax.rem(pair + k, pairs) + member, tp),
            device_id_type=MESH,
        )

    def state_arrival(k):
        slot = lax.rem(pair - k + pairs, pairs)
        return pltpu.make_async_remote_copy(
            src_ref=others.at[slot],
            dst_ref=others.at[slot],
            send_sem=state_s.at[k],
            recv_sem=state_r.at[k],
            device_id=(2 * slot + member, tp),
            device_id_type=MESH,
        )

    def parts_of(item):
        return (
            item[:depth_k],
            item[depth_k : depth_k + 1],
            item[depth_k + 1 : depth_k + 2],
            item[depth_k + 2 : depth_k + 3],
        )

    def join(earlier, later):
        decayed = earlier[2] + later[3]
        peak = jnp.maximum(decayed, later[2])
        keep = jnp.exp(decayed - peak)
        gain = jnp.exp(later[2] - peak)
        return (
            keep * earlier[0] + gain * later[0],
            keep * earlier[1] + gain * later[1],
            peak,
            earlier[3] + later[3],
        )

    mate_copy(member).start()
    launch_part(quarter, quarter)
    mate_copy(1 - member).wait_recv()
    for direction in range(2):
        for head in range(heads):
            joined = join(
                parts_of(both[direction, direction, head]),
                parts_of(both[1 - direction, direction, head]),
            )
            pair_sum[direction, head, :depth_k, :] = joined[0]
            for i in range(1, 4):
                pair_sum[direction, head, depth_k + i - 1 : depth_k + i, :] = joined[i]
            pair_sum[direction, head, depth_k + 3 :, :] = jnp.zeros((5, depth_v), jnp.float32)

    def send_state(k, carry):
        state_copy(k).start()
        return carry

    lax.fori_loop(1, pairs, send_state, 0)
    launch_part(2 * quarter, shard - 2 * quarter)
    launch(0, 1)

    def wait_state(k, carry):
        state_arrival(k).wait_recv()
        return carry

    lax.fori_loop(1, pairs, wait_state, 0)
    for direction in range(2):
        for head in range(heads):
            unit = direction * heads + head

            def take(j, carry):
                return join(carry, parts_of(others[j if direction == 0 else pairs - 1 - j, head]))

            def take_mate(j, carry):
                return join(carry, parts_of(both[direction, direction, head]))

            zero = jnp.zeros((1, BLOCK), jnp.float32)
            state = (jnp.zeros((depth_k, depth_v), jnp.float32), zero, zero, zero)
            state = lax.fori_loop(0, pair if direction == 0 else pairs - 1 - pair, take, state)
            state = lax.fori_loop(0, member if direction == 0 else 1 - member, take_mate, state)
            c_ref[unit] = jnp.zeros(c_ref.shape[1:], jnp.float32)
            c_ref[unit, head * depth_k : (head + 1) * depth_k, :] = state[0]
            n_ref[unit] = state[1]
            m_ref[unit] = state[2]

    def step(index, carry):
        for direction in range(2):
            block = index if direction == 0 else blocks - 1 - index
            rows = pl.ds(pl.multiple_of(block * BLOCK, BLOCK), BLOCK)
            query = q_ref[rows, :].astype(jnp.float32) * depth_k ** (-0.5)
            key = k_ref[rows, :]
            key_wide = key.astype(jnp.float32)
            cols = cols_ref[rows, :]
            keep = at_col <= at_row if direction == 0 else at_col >= at_row
            for head in range(heads):
                unit = direction * heads + head
                mine = (lane >= head * depth_k) & (lane < (head + 1) * depth_k)
                q_wide = jnp.where(mine, query, 0.0)
                q_own = q_wide.astype(jnp.bfloat16)
                value = v_ref[rows, head * depth_v : (head + 1) * depth_v]
                b_col = cols[:, unit : unit + 1]
                a_col = cols[:, units + unit : units + unit + 1]
                a_row = a_ref[pl.ds(block * units + unit, 1), :]
                total = total_ref[pl.ds(block * units + unit, 1), :]
                m_row = m_ref[unit]
                n_row = n_ref[unit]
                c_state = c_ref[unit]
                decay = jnp.where(keep, b_col + a_row, VERY_LOW)
                carry_log = b_col + m_row[:, :1]
                peak = jnp.maximum(carry_log, jnp.max(decay, axis=1, keepdims=True))
                scores = lax.dot_general(
                    q_own, key, (((1,), (1,)), ((), ())), preferred_element_type=jnp.float32
                ) * jnp.exp(decay - peak)
                carried = jnp.exp(carry_log - peak)
                number = two_pass(scores, value, ((1,), (0,)), True)
                number = number + carried * two_pass(q_own, c_state, ((1,), (0,)), False)
                below = jnp.sum(scores, axis=1, keepdims=True)
                below = below + carried * jnp.sum(q_wide * n_row, axis=1, keepdims=True)
                h_ref[direction, rows, head * depth_v : (head + 1) * depth_v] = number / jnp.maximum(
                    jnp.abs(below), jnp.exp(-peak)
                )
                new_m = jnp.maximum(total + m_row, total + jnp.max(a_row, axis=1, keepdims=True))
                shrink = jnp.exp(total + m_row - new_m)
                weight = jnp.exp(total[:, :1] + a_col - new_m[:, :1])
                weighted = weight * value.astype(jnp.float32)
                c_ref[unit] = shrink[:, :1] * c_state + two_pass(
                    key, weighted, ((0,), (0,)), False
                )
                n_ref[unit] = shrink[:, :1] * n_row + jnp.sum(
                    weight * key_wide, axis=0, keepdims=True
                )
                m_ref[unit] = new_m

        @pl.when(index == (2 * blocks) // 3)
        def _():
            advance(gu_events[0])

        return carry

    lax.fori_loop(0, blocks, step, 0)

    gain = gain_ref[...].astype(jnp.float32).reshape(1, wide_v)

    def finish(index, carry):
        rows = pl.ds(pl.multiple_of(index * BLOCK, BLOCK), BLOCK)
        for head in range(heads):
            span = slice(head * depth_v, (head + 1) * depth_v)
            summed = h_ref[0, rows, span] + h_ref[1, rows, span]
            scale = lax.rsqrt(jnp.mean(summed * summed, axis=1, keepdims=True) + EPSILON)
            opened = 1.0 / (1.0 + jnp.exp(-og_ref[rows, span].astype(jnp.float32)))
            place = pl.multiple_of(tp * wide_v + head * depth_v, depth_v)
            gated_all[rows, pl.ds(place, depth_v)] = (
                summed * scale * gain[:, span] * opened
            ).astype(jnp.bfloat16)
        return carry

    lax.fori_loop(0, blocks, finish, 0)
    for item in late:
        share(item)

    advance(gu_events[1])
    relay(("ow", 0))
    relay(("ng", 0))
    relay(early[2])
    relay(early[3])
    advance(gu_events[2])
    for item in early[4:]:
        relay(item)
    relay(late[0])
    advance(gu_events[3])
    for item in late[1:]:
        relay(item)
    for item in items:
        settle(item)
    for copy in own:
        copy.wait()

    norm_gain = ng_all[...].astype(jnp.float32).reshape(1, features)

    def project(index, carry):
        rows = pl.ds(pl.multiple_of(index * TILE, TILE), TILE)
        total = stream_all[rows, :].astype(jnp.float32) + jnp.dot(
            gated_all[rows, :], ow_all[...], preferred_element_type=jnp.float32
        )
        scale = lax.rsqrt(jnp.mean(total * total, axis=1, keepdims=True) + EPSILON)
        normed[rows, :] = (total * scale * norm_gain).astype(jnp.bfloat16)
        for j in range(features // width):

            @pl.when(tp == j)
            def _():
                res[rows, :] = total[:, j * width : (j + 1) * width]

        @pl.when(index == 2)
        def _():
            advance(gu_events[4])

        return carry

    lax.fori_loop(0, length // TILE, project, 0)
    for event in gu_events[5:]:
        advance(event)
    launch(2, 0)
    launch(2, 1)
    if reach >= 2:
        arrive(0, 1, reach - 2)
    arrive(0, 0, reach - 1)

    slab = 256
    part_rows = length // 2

    def activate(gate, up):
        return (gate / (1.0 + jnp.exp(-gate)) * up).astype(jnp.bfloat16)

    def open_slab(index, carry):
        first = pl.multiple_of(index * slab, slab)
        gate_cut = wgu[:, :, pl.ds(first, slab)].reshape(features, slab)
        up_cut = wgu[:, :, pl.ds(pl.multiple_of(hw + index * slab, BLOCK), slab)].reshape(
            features, slab
        )
        for part in range(2):
            rows = slice(part * part_rows, (part + 1) * part_rows)
            gate = jnp.dot(normed[rows, :], gate_cut, preferred_element_type=jnp.float32)
            up = jnp.dot(normed[rows, :], up_cut, preferred_element_type=jnp.float32)
            hidden[rows, pl.ds(first, slab)] = activate(gate, up)
        for at_slab, number in ((2, 0), (4, 1)):

            @pl.when(index == at_slab)
            def _():
                advance(d_events[number])

        return carry

    slabs = hw // slab
    lax.fori_loop(0, slabs, open_slab, 0)
    rest = hw - slabs * slab
    if rest:
        cut = jnp.concatenate(
            [wgu[:, :, slabs * slab : hw], wgu[:, :, hw + slabs * slab :]], axis=2
        ).reshape(features, 2 * rest)
        for part in range(2):
            rows = slice(part * part_rows, (part + 1) * part_rows)
            last = jnp.dot(normed[rows, :], cut, preferred_element_type=jnp.float32)
            hidden[rows, slabs * slab :] = activate(last[:, :rest], last[:, rest:])

    per_owner = width // PIECE
    by_arrival = shard == 2 * PIECE

    def stage(slot):
        return normed.at[:, pl.ds(pl.multiple_of(slot * PIECE, PIECE), PIECE)]

    def a_copy(slot):
        return pltpu.make_async_remote_copy(
            src_ref=stage(slot),
            dst_ref=recv_a.at[slot],
            send_sem=a_s.at[slot],
            recv_sem=a_r.at[slot],
            device_id=(sp, near),
            device_id_type=MESH,
        )

    def x_copy(slot):
        return pltpu.make_async_remote_copy(
            src_ref=stage(2 * per_owner + slot),
            dst_ref=recv_x.at[slot],
            send_sem=x_s.at[slot],
            recv_sem=x_r.at[slot],
            device_id=(sp, far),
            device_id_type=MESH,
        )

    if not by_arrival:
        for event in d_events[2:]:
            advance(event)
        arrive(2, 1, reach - 2)
        arrive(2, 0, reach - 1)

    def lower(index, carry):
        if by_arrival:
            hop = ((index + 1) // 2) * (1 - 2 * lax.rem(index, 2))
            sources = (at(pos + hop), at(pos - hop))
            for event in d_events[2:]:

                @pl.when(index == 2 * event[2] - 1 + event[1])
                def _():
                    advance(event)

            @pl.when(index == 2 * reach - 2)
            def _():
                arrive(2, 1, reach - 2)

            @pl.when(index == 2 * reach - 1)
            def _():
                arrive(2, 0, reach - 1)

            cut = jnp.concatenate([wd[sources[0], :PIECE, :], wd[sources[1], PIECE:, :]], axis=0)
            pieces = (2 * sources[0], 2 * sources[1] + 1)
        else:
            group = 2 * PIECE // shard
            cut = wd[pl.ds(pl.multiple_of(index * group, group), group)].reshape(2 * PIECE, hw)
            pieces = (2 * index, 2 * index + 1)
        product = lax.dot_general(
            hidden[...], cut, (((1,), (1,)), ((), ())), preferred_element_type=jnp.float32
        )
        parts = (product[:, :PIECE], product[:, PIECE:])
        roles = []
        for piece in pieces:
            owner = piece // per_owner
            low = lax.rem(lax.rem(tp, 2) + lax.rem(owner, 2), 2)
            high = lax.rem(tp // 2 + owner // 2, 2)
            roles.append((low, high, lax.rem(piece, per_owner)))

        for part, (low, high, slot) in zip(parts, roles):

            @pl.when(low == 1)
            def _():
                place = high * per_owner + slot
                first = pl.multiple_of(place * PIECE, PIECE)
                normed[:, pl.ds(first, PIECE)] = part.astype(jnp.bfloat16)
                a_copy(place).start()

            @pl.when((low == 0) & (high == 0))
            def _():
                first = pl.multiple_of(slot * PIECE, PIECE)
                res[:, pl.ds(first, PIECE)] = res[:, pl.ds(first, PIECE)] + part

        for part, (low, high, slot) in zip(parts, roles):

            @pl.when((low == 0) & (high == 1))
            def _():
                a_copy(per_owner + slot).wait_recv()
                first = pl.multiple_of((2 * per_owner + slot) * PIECE, PIECE)
                normed[:, pl.ds(first, PIECE)] = (
                    part + recv_a[per_owner + slot].astype(jnp.float32)
                ).astype(jnp.bfloat16)
                x_copy(slot).start()

        return carry

    lax.fori_loop(0, features // (2 * PIECE), lower, 0)

    outs = []
    for slot in range(per_owner):
        a_copy(slot).wait_recv()
        x_copy(slot).wait_recv()
        span = slice(slot * PIECE, (slot + 1) * PIECE)
        hidden[:, span] = (
            res[:, span] + recv_a[slot].astype(jnp.float32) + recv_x[slot].astype(jnp.float32)
        ).astype(jnp.bfloat16)
        outs.append(
            pltpu.make_async_copy(hidden.at[:, span], out_ref.at[:, span], local_s.at[10 + slot])
        )
        outs[-1].start()

    def state_left(k, carry):
        state_copy(k).wait_send()
        return carry

    lax.fori_loop(1, pairs, state_left, 0)
    mate_copy(member).wait_send()
    for base in (0, 2):
        for way in range(2):
            for turn in range(2):
                ring_copy(way, kind_of(way, base, turn), 0).wait_send()
        for _, turn, hop in events(base):
            for way in range(2):
                ring_copy(way, kind_of(way, base, turn), hop).wait_send()
    for item in items:
        for route in range(3):
            tp_copy(item, route).wait_send()
    for slot in range(2 * per_owner):
        a_copy(slot).wait_send()
    for slot in range(per_owner):
        x_copy(slot).wait_send()
    for copy in outs:
        copy.wait()


def local(
    query,
    key_rows,
    value,
    in_gate,
    forget_pre,
    out_gate,
    head_gain,
    out_weight,
    stream,
    norm_gain,
    gate_weight,
    up_weight,
    down_weight,
):
    length = query.shape[0]
    heads = in_gate.shape[1]
    depth_k = query.shape[1] // heads
    depth_v = value.shape[1] // heads
    blocks = length // BLOCK
    n_sp = lax.axis_size("sp")
    n_tp = lax.axis_size("tp")
    assert n_tp == 4 and n_sp % 2 == 0
    width = stream.shape[1]
    features = width * n_tp
    shard, hidden_width = gate_weight.shape
    units = 2 * heads
    chunks = next(c for c in (3, 2, 1) if blocks % c == 0)
    per_owner = width // PIECE
    reach = n_sp // 2
    wide_v = heads * depth_v
    dma = pltpu.SemaphoreType.DMA
    bf16, f32 = jnp.bfloat16, jnp.float32
    vmem = pl.BlockSpec(memory_space=pltpu.VMEM)
    anywhere = pl.BlockSpec(memory_space=pl.ANY)
    return pl.pallas_call(
        functools.partial(layer_kernel, n_sp, heads, chunks),
        out_shape=jax.ShapeDtypeStruct((length, width), bf16),
        in_specs=[vmem] * 3 + [anywhere] * 10,
        out_specs=anywhere,
        scratch_shapes=[
            pltpu.VMEM(query.shape, bf16),
            pltpu.VMEM(key_rows.shape, bf16),
            pltpu.VMEM(value.shape, bf16),
            pltpu.VMEM(out_gate.shape, bf16),
            pltpu.VMEM((blocks * units, BLOCK), f32),
            pltpu.VMEM((blocks * units, BLOCK), f32),
            pltpu.VMEM((blocks * units, BLOCK), f32),
            pltpu.VMEM((blocks * units, BLOCK), f32),
            pltpu.VMEM((length, 4 * units), f32),
            pltpu.VMEM((2, 2, heads, depth_k + 8, depth_v), f32),
            pltpu.VMEM((2, heads, depth_k + 8, depth_v), f32),
            pltpu.VMEM((n_sp, shard, 2 * hidden_width), bf16),
            pltpu.VMEM((n_sp, shard, hidden_width), bf16),
            pltpu.VMEM((n_tp * wide_v, features), bf16),
            pltpu.VMEM((length, features), bf16),
            pltpu.VMEM((length, n_tp * wide_v), bf16),
            pltpu.VMEM((features,), bf16),
            pltpu.VMEM((length, features), bf16),
            pltpu.VMEM((length, hidden_width), bf16),
            pltpu.VMEM((length, width), f32),
            pltpu.VMEM((2, length, wide_v), f32),
            pltpu.VMEM((units, heads * depth_k, depth_v), f32),
            pltpu.VMEM((units, 1, heads * depth_k), f32),
            pltpu.VMEM((units, 1, BLOCK), f32),
            pltpu.VMEM((n_sp // 2, heads, depth_k + 8, depth_v), f32),
            pltpu.VMEM((2 * per_owner, length, PIECE), bf16),
            pltpu.VMEM((per_owner, length, PIECE), bf16),
            dma((2, 4, reach)),
            dma((2, 4, reach)),
            dma,
            dma,
            dma((n_sp // 2,)),
            dma((n_sp // 2,)),
            dma((3, 2 + 2 * chunks)),
            dma((3, 2 + 2 * chunks)),
            dma((2 * per_owner,)),
            dma((2 * per_owner,)),
            dma((per_owner,)),
            dma((per_owner,)),
            dma((10 + per_owner,)),
        ],
        compiler_params=pltpu.CompilerParams(
            collective_id=0, has_side_effects=True, vmem_limit_bytes=67_000_000
        ),
        name="layer",
    )(
        in_gate,
        forget_pre,
        head_gain,
        query,
        key_rows,
        value,
        out_gate,
        norm_gain,
        stream,
        out_weight,
        gate_weight,
        up_weight,
        down_weight,
    )


def solution(mesh):
    placed = (
        P("sp", "tp"),
        P("sp", "tp"),
        P("sp", "tp"),
        P(None, "tp", "sp"),
        P(None, "tp", "sp"),
        P("sp", "tp"),
        P("tp"),
        P("tp", None),
        P("sp", "tp"),
        P("tp"),
        P("sp", "tp"),
        P("sp", "tp"),
        P("sp", "tp"),
    )
    return jax.shard_map(
        local, mesh=mesh, in_specs=placed, out_specs=P("sp", "tp"), check_vma=False
    )
```

```python
import functools

import jax
import jax.numpy as jnp
from jax import lax
from jax.experimental import pallas as pl
from jax.experimental.pallas import tpu as pltpu
from jax.sharding import PartitionSpec as P

BLOCK = 128
PIECE = 128
TILE = 256
HIGHEST = lax.Precision.HIGHEST
EPSILON = 1e-06
VERY_LOW = -1e30
MESH = pl.DeviceIdType.MESH


def two_pass(left, right, dims, split_left):
    wide = left if split_left else right
    high = wide.astype(jnp.bfloat16)
    low = (wide - high.astype(jnp.float32)).astype(jnp.bfloat16)
    total = None
    for part in (high, low):
        pair = (part, right) if split_left else (left, part)
        term = lax.dot_general(*pair, (dims, ((), ())), preferred_element_type=jnp.float32)
        total = term if total is None else total + term
    return total


def layer_kernel(
    n,
    heads,
    chunks,
    gate_in,
    forget_in,
    gain_ref,
    q_in,
    k_in,
    v_in,
    og_in,
    ng_ref,
    stream_ref,
    ow_ref,
    g_ref,
    u_ref,
    d_ref,
    out_ref,
    q_ref,
    k_ref,
    v_ref,
    og_ref,
    a_ref,
    b_ref,
    w_ref,
    total_ref,
    cols_ref,
    both,
    pair_sum,
    wgu,
    wd,
    ow_all,
    stream_all,
    gated_all,
    ng_all,
    normed,
    hidden,
    res,
    h_ref,
    c_ref,
    n_ref,
    m_ref,
    others,
    recv_a,
    recv_x,
    ring_s,
    ring_r,
    mate_s,
    mate_r,
    state_s,
    state_r,
    tp_s,
    tp_r,
    a_s,
    a_r,
    x_s,
    x_r,
    local_s,
):
    sp = lax.axis_index("sp")
    tp = lax.axis_index("tp")
    length = q_ref.shape[0]
    blocks = length // BLOCK
    units = 2 * heads
    depth_k = q_ref.shape[1] // heads
    depth_v = v_ref.shape[1] // heads
    wide_v = heads * depth_v
    width = stream_ref.shape[1]
    features = ow_ref.shape[1]
    shard, hw = d_ref.shape
    reach = n // 2

    near = tp + 1 - 2 * lax.rem(tp, 2)
    far = lax.rem(tp + 2, 4)
    cross = lax.rem(near + 2, 4)

    odd = lax.rem(sp, 2)
    pos = (1 - odd) * (sp // 2) + odd * (n - 1 - sp // 2)

    def at(place):
        place = lax.rem(place + 2 * n, n)
        second = place // (n // 2)
        return (1 - second) * 2 * place + second * (2 * (n - 1 - place) + 1)

    right, left = at(pos + 1), at(pos - 1)
    pairs = n // 2
    pair, member = sp // 2, lax.rem(sp, 2)
    mate = sp + 1 - 2 * member

    inputs = [
        pltpu.make_async_copy(source, target, local_s.at[6 + i])
        for i, (source, target) in enumerate(
            ((k_in, k_ref), (v_in, v_ref), (q_in, q_ref), (og_in, og_ref))
        )
    ]
    for copy in inputs:
        copy.start()

    barrier = pltpu.get_barrier_semaphore()

    def greet(k, carry):
        pl.semaphore_signal(
            barrier, inc=1, device_id=(lax.rem(sp + k, n), tp), device_id_type=MESH
        )
        return carry

    lax.fori_loop(1, n, greet, 0)
    for other in (near, far):
        pl.semaphore_signal(barrier, inc=1, device_id=(sp, other), device_id_type=MESH)
    pl.semaphore_wait(barrier, n + 1)

    half = shard // 2

    def slot_view(kind, source):
        if kind == 0:
            return wgu.at[source, :, pl.ds(0, hw)]
        if kind == 1:
            return wgu.at[source, :, pl.ds(hw, hw)]
        return wd.at[source, pl.ds((kind - 2) * half, half), :]

    def own_view(kind):
        if kind == 0:
            return g_ref
        if kind == 1:
            return u_ref
        return d_ref.at[pl.ds((kind - 2) * half, half), :]

    def ring_copy(way, kind, step):
        source = at(pos - step) if way == 0 else at(pos + step)
        return pltpu.make_async_remote_copy(
            src_ref=own_view(kind) if step == 0 else slot_view(kind, source),
            dst_ref=slot_view(kind, source),
            send_sem=ring_s.at[way, kind, step],
            recv_sem=ring_r.at[way, kind, step],
            device_id=(right if way == 0 else left, tp),
            device_id_type=MESH,
        )

    def ring_arrival(way, kind, step):
        source = at(pos - step - 1) if way == 0 else at(pos + step + 1)
        view = slot_view(kind, source)
        return pltpu.make_async_remote_copy(
            src_ref=view,
            dst_ref=view,
            send_sem=ring_s.at[way, kind, step],
            recv_sem=ring_r.at[way, kind, step],
            device_id=(right if way == 0 else left, tp),
            device_id_type=MESH,
        )

    def launch(base, turn):
        for way in range(2):
            ring_copy(way, kind_of(way, base, turn), 0).start()

    def launch_part(first, size):
        for way in range(2):
            rows = pl.ds(first, size)
            pltpu.make_async_remote_copy(
                src_ref=own_view(way).at[rows, :],
                dst_ref=wgu.at[sp, rows, pl.ds(way * hw, hw)],
                send_sem=ring_s.at[way, way, 0],
                recv_sem=ring_r.at[way, way, 0],
                device_id=(right if way == 0 else left, tp),
                device_id_type=MESH,
            ).start()

    quarter = shard // 4

    def kind_of(way, base, turn):
        return base + (turn if way == 0 else 1 - turn)

    def arrive(base, turn, step):
        for way in range(2):
            ring_arrival(way, kind_of(way, base, turn), step).wait_recv()

    def advance(event):
        base, turn, step = event
        for way in range(2):
            kind = kind_of(way, base, turn)
            ring_arrival(way, kind, step - 1).wait_recv()
            ring_copy(way, kind, step).start()

    def events(base):
        return [(base, turn, step) for step in range(1, reach) for turn in range(2)][:-1]

    gu_events = events(0)
    d_events = events(2)
    launch_part(0, quarter)

    chunk = length // chunks
    items = [("ow", 0), ("ng", 0)]
    items += [("stream", i) for i in range(chunks)]
    items += [("gated", i) for i in range(chunks)]

    def tp_view(item, slot):
        what, i = item
        if what == "ow":
            return ow_all.at[pl.ds(pl.multiple_of(slot * wide_v, wide_v), wide_v), :]
        if what == "ng":
            return ng_all.at[pl.ds(pl.multiple_of(slot * width, width), width)]
        if what == "stream":
            return stream_all.at[
                pl.ds(i * chunk, chunk), pl.ds(pl.multiple_of(slot * width, width), width)
            ]
        return gated_all.at[
            pl.ds(i * chunk, chunk), pl.ds(pl.multiple_of(slot * wide_v, wide_v), wide_v)
        ]

    def tp_own(item):
        what, i = item
        if what == "ow":
            return ow_ref
        if what == "ng":
            return ng_ref
        if what == "stream":
            return stream_ref.at[pl.ds(i * chunk, chunk), :]
        return tp_view(item, tp)

    def tp_copy(item, route):
        number = items.index(item)
        slot = tp if route < 2 else far
        return pltpu.make_async_remote_copy(
            src_ref=tp_own(item) if route < 2 else tp_view(item, far),
            dst_ref=tp_view(item, slot),
            send_sem=tp_s.at[route, number],
            recv_sem=tp_r.at[route, number],
            device_id=(sp, far if route == 0 else near),
            device_id_type=MESH,
        )

    def tp_arrival(item, route):
        number = items.index(item)
        view = tp_view(item, (far, near, cross)[route])
        return pltpu.make_async_remote_copy(
            src_ref=view,
            dst_ref=view,
            send_sem=tp_s.at[route, number],
            recv_sem=tp_r.at[route, number],
            device_id=(sp, far if route == 0 else near),
            device_id_type=MESH,
        )

    def share(item):
        for route in range(2):
            tp_copy(item, route).start()

    def relay(item):
        tp_arrival(item, 0).wait_recv()
        tp_copy(item, 2).start()

    def settle(item):
        for route in (1, 2):
            tp_arrival(item, route).wait_recv()

    early = items[: 2 + chunks]
    late = items[2 + chunks :]
    for item in early:
        share(item)

    own = [
        pltpu.make_async_copy(g_ref, slot_view(0, sp), local_s.at[0]),
        pltpu.make_async_copy(u_ref, slot_view(1, sp), local_s.at[1]),
        pltpu.make_async_copy(d_ref, wd.at[sp], local_s.at[2]),
        pltpu.make_async_copy(ow_ref, tp_view(("ow", 0), tp), local_s.at[3]),
        pltpu.make_async_copy(
            stream_ref,
            stream_all.at[:, pl.ds(pl.multiple_of(tp * width, width), width)],
            local_s.at[4],
        ),
        pltpu.make_async_copy(ng_ref, tp_view(("ng", 0), tp), local_s.at[5]),
    ]
    for copy in own:
        copy.start()

    both[member] = jnp.zeros(both.shape[1:], jnp.float32)

    for copy in inputs:
        copy.wait()
    for block in range(blocks):
        for unit in range(units):
            spot = block * units + unit
            tokens = slice(block * BLOCK, (block + 1) * BLOCK)
            a_ref[spot : spot + 1, :] = gate_in[unit // heads, unit % heads : unit % heads + 1, tokens]
            b_ref[spot : spot + 1, :] = forget_in[
                unit // heads, unit % heads : unit % heads + 1, tokens
            ]
    raw = b_ref[...]
    forgets = jnp.minimum(raw, 0.0) - jnp.log1p(jnp.exp(-jnp.abs(raw)))
    at_row = lax.broadcasted_iota(jnp.int32, (BLOCK, BLOCK), 0)
    at_col = lax.broadcasted_iota(jnp.int32, (BLOCK, BLOCK), 1)
    upto = (at_row <= at_col).astype(jnp.bfloat16)
    since = (at_row >= at_col).astype(jnp.bfloat16)
    first = forgets.astype(jnp.bfloat16)
    left_over = forgets - first.astype(jnp.float32)
    second = left_over.astype(jnp.bfloat16)
    third = (left_over - second.astype(jnp.float32)).astype(jnp.bfloat16)
    ahead = jnp.zeros_like(forgets)
    behind = jnp.zeros_like(forgets)
    for piece in (third, second, first):
        ahead = ahead + jnp.dot(piece, upto, preferred_element_type=jnp.float32)
        behind = behind + jnp.dot(piece, since, preferred_element_type=jnp.float32)
    spots = lax.broadcasted_iota(jnp.int32, forgets.shape, 0)
    sums = jnp.where(lax.rem(spots, units) < heads, ahead, behind)
    shifted = a_ref[...] - sums
    b_ref[...] = sums
    a_ref[...] = shifted
    total_ref[...] = jnp.broadcast_to(jnp.sum(forgets, axis=1, keepdims=True), forgets.shape)
    peaks = []
    for unit in range(units):
        direction = unit // heads
        beyond = jnp.zeros((1, BLOCK), jnp.float32)
        order = range(blocks - 1, -1, -1) if direction == 0 else range(blocks)
        highest = None
        for block in order:
            spot = block * units + unit
            beyond = beyond + total_ref[spot : spot + 1, :]
            logs = beyond + a_ref[spot : spot + 1, :]
            w_ref[spot : spot + 1, :] = logs
            highest = logs if highest is None else jnp.maximum(highest, logs)
        highest = jnp.broadcast_to(jnp.max(highest, axis=1, keepdims=True), (1, BLOCK))
        peaks.append(highest)
        head = unit % heads
        both[member, direction, head, depth_k + 1 : depth_k + 2, :] = highest
        both[member, direction, head, depth_k + 2 : depth_k + 3, :] = beyond
    for block in range(blocks):
        spot = slice(block * units, (block + 1) * units)
        w_ref[spot, :] = jnp.exp(w_ref[spot, :] - jnp.concatenate(peaks, axis=0))

    lane = lax.broadcasted_iota(jnp.int32, (BLOCK, q_ref.shape[1]), 1)
    lane_row = lax.broadcasted_iota(jnp.int32, (1, q_ref.shape[1]), 1)

    def turn_block(block, normers):
        rows = pl.ds(pl.multiple_of(block * BLOCK, BLOCK), BLOCK)
        spot = pl.ds(block * units, units)
        stacked = jnp.concatenate([b_ref[spot, :], a_ref[spot, :], w_ref[spot, :], w_ref[spot, :]], axis=0)
        columns = stacked.T
        cols_ref[rows, : 4 * units] = columns
        key_wide = k_ref[rows, :].astype(jnp.float32)
        out = []
        for unit in range(units):
            head = unit % heads
            weight = columns[:, 2 * units + unit : 2 * units + unit + 1]
            value = v_ref[rows, head * depth_v : (head + 1) * depth_v].astype(jnp.float32)
            hidden[rows, unit * depth_v : (unit + 1) * depth_v] = (weight * value).astype(jnp.bfloat16)
            out.append(normers[unit] + jnp.sum(weight * key_wide, axis=0, keepdims=True))
        return tuple(out)

    normers = lax.fori_loop(
        0,
        blocks,
        turn_block,
        tuple(jnp.zeros((1, heads * depth_k), jnp.float32) for _ in range(units)),
    )
    outer = lax.dot_general(
        k_ref[...],
        hidden[:, : units * depth_v],
        (((0,), (0,)), ((), ())),
        preferred_element_type=jnp.float32,
    )
    for unit in range(units):
        direction, head = unit // heads, unit % heads
        both[member, direction, head, :depth_k, :] = outer[
            head * depth_k : (head + 1) * depth_k, unit * depth_v : (unit + 1) * depth_v
        ]
        mine = (lane_row >= head * depth_k) & (lane_row < (head + 1) * depth_k)
        both[member, direction, head, depth_k : depth_k + 1, :] = jnp.where(mine, normers[unit], 0.0)

    def mate_copy(which):
        return pltpu.make_async_remote_copy(
            src_ref=both.at[which],
            dst_ref=both.at[which],
            send_sem=mate_s,
            recv_sem=mate_r,
            device_id=(mate, tp),
            device_id_type=MESH,
        )

    def state_copy(k):
        return pltpu.make_async_remote_copy(
            src_ref=pair_sum.at[(pair + k) // pairs],
            dst_ref=others.at[pair],
            send_sem=state_s.at[k],
            recv_sem=state_r.at[k],
            device_id=(2 * lax.rem(pair + k, pairs) + member, tp),
            device_id_type=MESH,
        )

    def state_arrival(k):
        slot = lax.rem(pair - k + pairs, pairs)
        return pltpu.make_async_remote_copy(
            src_ref=others.at[slot],
            dst_ref=others.at[slot],
            send_sem=state_s.at[k],
            recv_sem=state_r.at[k],
            device_id=(2 * slot + member, tp),
            device_id_type=MESH,
        )

    def parts_of(item):
        return (
            item[:depth_k],
            item[depth_k : depth_k + 1],
            item[depth_k + 1 : depth_k + 2],
            item[depth_k + 2 : depth_k + 3],
        )

    def join(earlier, later):
        decayed = earlier[2] + later[3]
        peak = jnp.maximum(decayed, later[2])
        keep = jnp.exp(decayed - peak)
        gain = jnp.exp(later[2] - peak)
        return (
            keep * earlier[0] + gain * later[0],
            keep * earlier[1] + gain * later[1],
            peak,
            earlier[3] + later[3],
        )

    mate_copy(member).start()
    launch_part(quarter, quarter)
    mate_copy(1 - member).wait_recv()
    for direction in range(2):
        for head in range(heads):
            joined = join(
                parts_of(both[direction, direction, head]),
                parts_of(both[1 - direction, direction, head]),
            )
            pair_sum[direction, head, :depth_k, :] = joined[0]
            for i in range(1, 4):
                pair_sum[direction, head, depth_k + i - 1 : depth_k + i, :] = joined[i]
            pair_sum[direction, head, depth_k + 3 :, :] = jnp.zeros((5, depth_v), jnp.float32)

    def send_state(k, carry):
        state_copy(k).start()
        return carry

    lax.fori_loop(1, pairs, send_state, 0)
    launch_part(2 * quarter, shard - 2 * quarter)
    launch(0, 1)

    def wait_state(k, carry):
        state_arrival(k).wait_recv()
        return carry

    lax.fori_loop(1, pairs, wait_state, 0)
    for direction in range(2):
        for head in range(heads):
            unit = direction * heads + head

            def take(j, carry):
                return join(carry, parts_of(others[j if direction == 0 else pairs - 1 - j, head]))

            def take_mate(j, carry):
                return join(carry, parts_of(both[direction, direction, head]))

            zero = jnp.zeros((1, BLOCK), jnp.float32)
            state = (jnp.zeros((depth_k, depth_v), jnp.float32), zero, zero, zero)
            state = lax.fori_loop(0, pair if direction == 0 else pairs - 1 - pair, take, state)
            state = lax.fori_loop(0, member if direction == 0 else 1 - member, take_mate, state)
            c_ref[unit] = jnp.zeros(c_ref.shape[1:], jnp.float32)
            c_ref[unit, head * depth_k : (head + 1) * depth_k, :] = state[0]
            n_ref[unit] = state[1]
            m_ref[unit] = state[2]

    def step(index, carry):
        for direction in range(2):
            block = index if direction == 0 else blocks - 1 - index
            rows = pl.ds(pl.multiple_of(block * BLOCK, BLOCK), BLOCK)
            query = q_ref[rows, :].astype(jnp.float32) * depth_k ** (-0.5)
            key = k_ref[rows, :]
            key_wide = key.astype(jnp.float32)
            cols = cols_ref[rows, :]
            keep = at_col <= at_row if direction == 0 else at_col >= at_row
            for head in range(heads):
                unit = direction * heads + head
                mine = (lane >= head * depth_k) & (lane < (head + 1) * depth_k)
                q_wide = jnp.where(mine, query, 0.0)
                q_own = q_wide.astype(jnp.bfloat16)
                value = v_ref[rows, head * depth_v : (head + 1) * depth_v]
                b_col = cols[:, unit : unit + 1]
                a_col = cols[:, units + unit : units + unit + 1]
                a_row = a_ref[pl.ds(block * units + unit, 1), :]
                total = total_ref[pl.ds(block * units + unit, 1), :]
                m_row = m_ref[unit]
                n_row = n_ref[unit]
                c_state = c_ref[unit]
                decay = jnp.where(keep, b_col + a_row, VERY_LOW)
                carry_log = b_col + m_row[:, :1]
                peak = jnp.maximum(carry_log, jnp.max(decay, axis=1, keepdims=True))
                scores = lax.dot_general(
                    q_own, key, (((1,), (1,)), ((), ())), preferred_element_type=jnp.float32
                ) * jnp.exp(decay - peak)
                carried = jnp.exp(carry_log - peak)
                number = two_pass(scores, value, ((1,), (0,)), True)
                number = number + carried * two_pass(q_own, c_state, ((1,), (0,)), False)
                below = jnp.sum(scores, axis=1, keepdims=True)
                below = below + carried * jnp.sum(q_wide * n_row, axis=1, keepdims=True)
                h_ref[direction, rows, head * depth_v : (head + 1) * depth_v] = number / jnp.maximum(
                    jnp.abs(below), jnp.exp(-peak)
                )
                new_m = jnp.maximum(total + m_row, total + jnp.max(a_row, axis=1, keepdims=True))
                shrink = jnp.exp(total + m_row - new_m)
                weight = jnp.exp(total[:, :1] + a_col - new_m[:, :1])
                weighted = weight * value.astype(jnp.float32)
                c_ref[unit] = shrink[:, :1] * c_state + two_pass(
                    key, weighted, ((0,), (0,)), False
                )
                n_ref[unit] = shrink[:, :1] * n_row + jnp.sum(
                    weight * key_wide, axis=0, keepdims=True
                )
                m_ref[unit] = new_m

        @pl.when(index == (2 * blocks) // 3)
        def _():
            advance(gu_events[0])

        return carry

    lax.fori_loop(0, blocks, step, 0)

    gain = gain_ref[...].astype(jnp.float32).reshape(1, wide_v)

    def finish(index, carry):
        rows = pl.ds(pl.multiple_of(index * BLOCK, BLOCK), BLOCK)
        for head in range(heads):
            span = slice(head * depth_v, (head + 1) * depth_v)
            summed = h_ref[0, rows, span] + h_ref[1, rows, span]
            scale = lax.rsqrt(jnp.mean(summed * summed, axis=1, keepdims=True) + EPSILON)
            opened = 1.0 / (1.0 + jnp.exp(-og_ref[rows, span].astype(jnp.float32)))
            place = pl.multiple_of(tp * wide_v + head * depth_v, depth_v)
            gated_all[rows, pl.ds(place, depth_v)] = (
                summed * scale * gain[:, span] * opened
            ).astype(jnp.bfloat16)
        return carry

    lax.fori_loop(0, blocks, finish, 0)
    for item in late:
        share(item)

    advance(gu_events[1])
    relay(("ow", 0))
    relay(("ng", 0))
    relay(early[2])
    relay(early[3])
    advance(gu_events[2])
    for item in early[4:]:
        relay(item)
    relay(late[0])
    advance(gu_events[3])
    for item in late[1:]:
        relay(item)
    for item in items:
        settle(item)
    for copy in own:
        copy.wait()

    norm_gain = ng_all[...].astype(jnp.float32).reshape(1, features)

    def project(index, carry):
        rows = pl.ds(pl.multiple_of(index * TILE, TILE), TILE)
        total = stream_all[rows, :].astype(jnp.float32) + jnp.dot(
            gated_all[rows, :], ow_all[...], preferred_element_type=jnp.float32
        )
        scale = lax.rsqrt(jnp.mean(total * total, axis=1, keepdims=True) + EPSILON)
        normed[rows, :] = (total * scale * norm_gain).astype(jnp.bfloat16)
        for j in range(features // width):

            @pl.when(tp == j)
            def _():
                res[rows, :] = total[:, j * width : (j + 1) * width]

        @pl.when(index == 2)
        def _():
            advance(gu_events[4])

        return carry

    lax.fori_loop(0, length // TILE, project, 0)
    for event in gu_events[5:]:
        advance(event)
    launch(2, 0)
    launch(2, 1)
    if reach >= 2:
        arrive(0, 1, reach - 2)
    arrive(0, 0, reach - 1)

    slab = 256
    part_rows = length // 2

    def activate(gate, up):
        return (gate / (1.0 + jnp.exp(-gate)) * up).astype(jnp.bfloat16)

    def open_slab(index, carry):
        first = pl.multiple_of(index * slab, slab)
        gate_cut = wgu[:, :, pl.ds(first, slab)].reshape(features, slab)
        up_cut = wgu[:, :, pl.ds(pl.multiple_of(hw + index * slab, BLOCK), slab)].reshape(
            features, slab
        )
        for part in range(2):
            rows = slice(part * part_rows, (part + 1) * part_rows)
            gate = jnp.dot(normed[rows, :], gate_cut, preferred_element_type=jnp.float32)
            up = jnp.dot(normed[rows, :], up_cut, preferred_element_type=jnp.float32)
            hidden[rows, pl.ds(first, slab)] = activate(gate, up)
        for at_slab, number in ((2, 0), (4, 1)):

            @pl.when(index == at_slab)
            def _():
                advance(d_events[number])

        return carry

    slabs = hw // slab
    lax.fori_loop(0, slabs, open_slab, 0)
    rest = hw - slabs * slab
    if rest:
        cut = jnp.concatenate(
            [wgu[:, :, slabs * slab : hw], wgu[:, :, hw + slabs * slab :]], axis=2
        ).reshape(features, 2 * rest)
        for part in range(2):
            rows = slice(part * part_rows, (part + 1) * part_rows)
            last = jnp.dot(normed[rows, :], cut, preferred_element_type=jnp.float32)
            hidden[rows, slabs * slab :] = activate(last[:, :rest], last[:, rest:])

    per_owner = width // PIECE
    by_arrival = shard == 2 * PIECE and per_owner == 4

    def stage(slot):
        return normed.at[:, pl.ds(pl.multiple_of(slot * PIECE, PIECE), PIECE)]

    def a_copy(slot):
        return pltpu.make_async_remote_copy(
            src_ref=stage(slot),
            dst_ref=recv_a.at[slot],
            send_sem=a_s.at[slot],
            recv_sem=a_r.at[slot],
            device_id=(sp, near),
            device_id_type=MESH,
        )

    def x_copy(slot):
        return pltpu.make_async_remote_copy(
            src_ref=stage(2 * per_owner + slot),
            dst_ref=recv_x.at[slot],
            send_sem=x_s.at[slot],
            recv_sem=x_r.at[slot],
            device_id=(sp, far),
            device_id_type=MESH,
        )

    if not by_arrival:
        for event in d_events[2:]:
            advance(event)
        arrive(2, 1, reach - 2)
        arrive(2, 0, reach - 1)

    def lower(index, carry):
        if by_arrival:
            hop = ((index + 1) // 2) * (1 - 2 * lax.rem(index, 2))
            sources = (at(pos + hop), at(pos - hop))
            for event in d_events[2:]:

                @pl.when(index == 2 * event[2] - 1 + event[1])
                def _():
                    advance(event)

            @pl.when(index == 2 * reach - 2)
            def _():
                arrive(2, 1, reach - 2)

            @pl.when(index == 2 * reach - 1)
            def _():
                arrive(2, 0, reach - 1)

            cut = jnp.concatenate([wd[sources[0], :PIECE, :], wd[sources[1], PIECE:, :]], axis=0)
            pieces = (2 * sources[0], 2 * sources[1] + 1)
        else:
            group = 2 * PIECE // shard
            cut = wd[pl.ds(pl.multiple_of(index * group, group), group)].reshape(2 * PIECE, hw)
            pieces = (2 * index, 2 * index + 1)
        product = lax.dot_general(
            hidden[...], cut, (((1,), (1,)), ((), ())), preferred_element_type=jnp.float32
        )
        parts = (product[:, :PIECE], product[:, PIECE:])
        roles = []
        for piece in pieces:
            owner = piece // per_owner
            low = lax.rem(lax.rem(tp, 2) + lax.rem(owner, 2), 2)
            high = lax.rem(tp // 2 + owner // 2, 2)
            roles.append((low, high, lax.rem(piece, per_owner)))

        for part, (low, high, slot) in zip(parts, roles):

            @pl.when(low == 1)
            def _():
                place = high * per_owner + slot
                first = pl.multiple_of(place * PIECE, PIECE)
                normed[:, pl.ds(first, PIECE)] = part.astype(jnp.bfloat16)
                a_copy(place).start()

            @pl.when((low == 0) & (high == 0))
            def _():
                first = pl.multiple_of(slot * PIECE, PIECE)
                res[:, pl.ds(first, PIECE)] = res[:, pl.ds(first, PIECE)] + part

        for part, (low, high, slot) in zip(parts, roles):

            @pl.when((low == 0) & (high == 1))
            def _():
                a_copy(per_owner + slot).wait_recv()
                first = pl.multiple_of((2 * per_owner + slot) * PIECE, PIECE)
                normed[:, pl.ds(first, PIECE)] = (
                    part + recv_a[per_owner + slot].astype(jnp.float32)
                ).astype(jnp.bfloat16)
                x_copy(slot).start()

        return carry

    lax.fori_loop(0, features // (2 * PIECE), lower, 0)

    for turn in range(per_owner):
        if by_arrival:
            hops_even = lax.rem(pos - tp + n, n)
            hops_odd = lax.rem(pos + 1 + tp, n)
            far_even = reach - jnp.abs(reach - hops_even)
            far_odd = reach - jnp.abs(reach - hops_odd)
            late = (far_even > far_odd).astype(jnp.int32)
            side = late + (turn // 2) * (1 - 2 * late)
            slot = 2 * side + turn % 2
        else:
            slot = turn
        a_copy(slot).wait_recv()
        x_copy(slot).wait_recv()
        span = pl.ds(pl.multiple_of(slot * PIECE, PIECE), PIECE)
        out_ref[:, span] = (
            res[:, span] + recv_a[slot].astype(jnp.float32) + recv_x[slot].astype(jnp.float32)
        ).astype(jnp.bfloat16)

    def state_left(k, carry):
        state_copy(k).wait_send()
        return carry

    lax.fori_loop(1, pairs, state_left, 0)
    mate_copy(member).wait_send()
    for base in (0, 2):
        for way in range(2):
            for turn in range(2):
                ring_copy(way, kind_of(way, base, turn), 0).wait_send()
        for _, turn, hop in events(base):
            for way in range(2):
                ring_copy(way, kind_of(way, base, turn), hop).wait_send()
    for item in items:
        for route in range(3):
            tp_copy(item, route).wait_send()
    for slot in range(2 * per_owner):
        a_copy(slot).wait_send()
    for slot in range(per_owner):
        x_copy(slot).wait_send()


def local(
    query,
    key_rows,
    value,
    in_gate,
    forget_pre,
    out_gate,
    head_gain,
    out_weight,
    stream,
    norm_gain,
    gate_weight,
    up_weight,
    down_weight,
):
    length = query.shape[0]
    heads = in_gate.shape[1]
    depth_k = query.shape[1] // heads
    depth_v = value.shape[1] // heads
    blocks = length // BLOCK
    n_sp = lax.axis_size("sp")
    n_tp = lax.axis_size("tp")
    assert n_tp == 4 and n_sp % 2 == 0
    width = stream.shape[1]
    features = width * n_tp
    shard, hidden_width = gate_weight.shape
    units = 2 * heads
    chunks = next(c for c in (3, 2, 1) if blocks % c == 0)
    per_owner = width // PIECE
    reach = n_sp // 2
    wide_v = heads * depth_v
    dma = pltpu.SemaphoreType.DMA
    bf16, f32 = jnp.bfloat16, jnp.float32
    vmem = pl.BlockSpec(memory_space=pltpu.VMEM)
    anywhere = pl.BlockSpec(memory_space=pl.ANY)
    return pl.pallas_call(
        functools.partial(layer_kernel, n_sp, heads, chunks),
        out_shape=pltpu.VMEM((length, width), bf16),
        in_specs=[vmem] * 3 + [anywhere] * 10,
        out_specs=vmem,
        scratch_shapes=[
            pltpu.VMEM(query.shape, bf16),
            pltpu.VMEM(key_rows.shape, bf16),
            pltpu.VMEM(value.shape, bf16),
            pltpu.VMEM(out_gate.shape, bf16),
            pltpu.VMEM((blocks * units, BLOCK), f32),
            pltpu.VMEM((blocks * units, BLOCK), f32),
            pltpu.VMEM((blocks * units, BLOCK), f32),
            pltpu.VMEM((blocks * units, BLOCK), f32),
            pltpu.VMEM((length, 4 * units), f32),
            pltpu.VMEM((2, 2, heads, depth_k + 8, depth_v), f32),
            pltpu.VMEM((2, heads, depth_k + 8, depth_v), f32),
            pltpu.VMEM((n_sp, shard, 2 * hidden_width), bf16),
            pltpu.VMEM((n_sp, shard, hidden_width), bf16),
            pltpu.VMEM((n_tp * wide_v, features), bf16),
            pltpu.VMEM((length, features), bf16),
            pltpu.VMEM((length, n_tp * wide_v), bf16),
            pltpu.VMEM((features,), bf16),
            pltpu.VMEM((length, features), bf16),
            pltpu.VMEM((length, hidden_width), bf16),
            pltpu.VMEM((length, width), f32),
            pltpu.VMEM((2, length, wide_v), f32),
            pltpu.VMEM((units, heads * depth_k, depth_v), f32),
            pltpu.VMEM((units, 1, heads * depth_k), f32),
            pltpu.VMEM((units, 1, BLOCK), f32),
            pltpu.VMEM((n_sp // 2, heads, depth_k + 8, depth_v), f32),
            pltpu.VMEM((2 * per_owner, length, PIECE), bf16),
            pltpu.VMEM((per_owner, length, PIECE), bf16),
            dma((2, 4, reach)),
            dma((2, 4, reach)),
            dma,
            dma,
            dma((n_sp // 2,)),
            dma((n_sp // 2,)),
            dma((3, 2 + 2 * chunks)),
            dma((3, 2 + 2 * chunks)),
            dma((2 * per_owner,)),
            dma((2 * per_owner,)),
            dma((per_owner,)),
            dma((per_owner,)),
            dma((10,)),
        ],
        compiler_params=pltpu.CompilerParams(
            collective_id=0, has_side_effects=True, vmem_limit_bytes=65_000_000
        ),
        name="layer",
    )(
        in_gate,
        forget_pre,
        head_gain,
        query,
        key_rows,
        value,
        out_gate,
        norm_gain,
        stream,
        out_weight,
        gate_weight,
        up_weight,
        down_weight,
    )


def solution(mesh):
    placed = (
        P("sp", "tp"),
        P("sp", "tp"),
        P("sp", "tp"),
        P(None, "tp", "sp"),
        P(None, "tp", "sp"),
        P("sp", "tp"),
        P("tp"),
        P("tp", None),
        P("sp", "tp"),
        P("tp"),
        P("sp", "tp"),
        P("sp", "tp"),
        P("sp", "tp"),
    )
    return jax.shard_map(
        local, mesh=mesh, in_specs=placed, out_specs=P("sp", "tp"), check_vma=False
    )
```

```python
import functools

import jax
import jax.numpy as jnp
from jax import lax
from jax.experimental import pallas as pl
from jax.experimental.pallas import tpu as pltpu
from jax.sharding import PartitionSpec as P

BLOCK = 128
PIECE = 128
TILE = 256
HIGHEST = lax.Precision.HIGHEST
EPSILON = 1e-06
VERY_LOW = -1e30
MESH = pl.DeviceIdType.MESH


def two_pass(left, right, dims, split_left):
    wide = left if split_left else right
    high = wide.astype(jnp.bfloat16)
    low = (wide - high.astype(jnp.float32)).astype(jnp.bfloat16)
    total = None
    for part in (high, low):
        pair = (part, right) if split_left else (left, part)
        term = lax.dot_general(*pair, (dims, ((), ())), preferred_element_type=jnp.float32)
        total = term if total is None else total + term
    return total


def layer_kernel(
    n,
    heads,
    chunks,
    gate_in,
    forget_in,
    gain_ref,
    q_in,
    k_in,
    v_in,
    og_in,
    ng_ref,
    stream_ref,
    ow_ref,
    g_ref,
    u_ref,
    d_ref,
    out_ref,
    q_ref,
    k_ref,
    v_ref,
    og_ref,
    a_ref,
    b_ref,
    w_ref,
    total_ref,
    cols_ref,
    both,
    pair_sum,
    wgu,
    wd,
    ow_all,
    stream_all,
    gated_all,
    ng_all,
    normed,
    hidden,
    res,
    h_ref,
    c_ref,
    n_ref,
    m_ref,
    others,
    recv_a,
    recv_x,
    ring_s,
    ring_r,
    mate_s,
    mate_r,
    state_s,
    state_r,
    tp_s,
    tp_r,
    a_s,
    a_r,
    x_s,
    x_r,
    local_s,
):
    sp = lax.axis_index("sp")
    tp = lax.axis_index("tp")
    length = q_ref.shape[0]
    blocks = length // BLOCK
    units = 2 * heads
    depth_k = q_ref.shape[1] // heads
    depth_v = v_ref.shape[1] // heads
    wide_v = heads * depth_v
    width = stream_ref.shape[1]
    features = ow_ref.shape[1]
    shard, hw = d_ref.shape
    reach = n // 2

    near = tp + 1 - 2 * lax.rem(tp, 2)
    far = lax.rem(tp + 2, 4)
    cross = lax.rem(near + 2, 4)

    odd = lax.rem(sp, 2)
    pos = (1 - odd) * (sp // 2) + odd * (n - 1 - sp // 2)

    def at(place):
        place = lax.rem(place + 2 * n, n)
        second = place // (n // 2)
        return (1 - second) * 2 * place + second * (2 * (n - 1 - place) + 1)

    right, left = at(pos + 1), at(pos - 1)
    pairs = n // 2
    pair, member = sp // 2, lax.rem(sp, 2)
    mate = sp + 1 - 2 * member

    inputs = [
        pltpu.make_async_copy(source, target, local_s.at[6 + i])
        for i, (source, target) in enumerate(
            ((k_in, k_ref), (v_in, v_ref), (q_in, q_ref), (og_in, og_ref))
        )
    ]
    for copy in inputs:
        copy.start()

    barrier = pltpu.get_barrier_semaphore()

    def greet(k, carry):
        pl.semaphore_signal(
            barrier, inc=1, device_id=(lax.rem(sp + k, n), tp), device_id_type=MESH
        )
        return carry

    lax.fori_loop(1, n, greet, 0)
    for other in (near, far):
        pl.semaphore_signal(barrier, inc=1, device_id=(sp, other), device_id_type=MESH)
    pl.semaphore_wait(barrier, n + 1)

    half = shard // 2

    def slot_view(kind, source):
        if kind == 0:
            return wgu.at[source, :, pl.ds(0, hw)]
        if kind == 1:
            return wgu.at[source, :, pl.ds(hw, hw)]
        return wd.at[source, pl.ds((kind - 2) * half, half), :]

    def own_view(kind):
        if kind == 0:
            return g_ref
        if kind == 1:
            return u_ref
        return d_ref.at[pl.ds((kind - 2) * half, half), :]

    def ring_copy(way, kind, step):
        source = at(pos - step) if way == 0 else at(pos + step)
        return pltpu.make_async_remote_copy(
            src_ref=own_view(kind) if step == 0 else slot_view(kind, source),
            dst_ref=slot_view(kind, source),
            send_sem=ring_s.at[way, kind, step],
            recv_sem=ring_r.at[way, kind, step],
            device_id=(right if way == 0 else left, tp),
            device_id_type=MESH,
        )

    def ring_arrival(way, kind, step):
        source = at(pos - step - 1) if way == 0 else at(pos + step + 1)
        view = slot_view(kind, source)
        return pltpu.make_async_remote_copy(
            src_ref=view,
            dst_ref=view,
            send_sem=ring_s.at[way, kind, step],
            recv_sem=ring_r.at[way, kind, step],
            device_id=(right if way == 0 else left, tp),
            device_id_type=MESH,
        )

    def launch(base, turn):
        for way in range(2):
            ring_copy(way, kind_of(way, base, turn), 0).start()

    def launch_part(first, size):
        for way in range(2):
            rows = pl.ds(first, size)
            pltpu.make_async_remote_copy(
                src_ref=own_view(way).at[rows, :],
                dst_ref=wgu.at[sp, rows, pl.ds(way * hw, hw)],
                send_sem=ring_s.at[way, way, 0],
                recv_sem=ring_r.at[way, way, 0],
                device_id=(right if way == 0 else left, tp),
                device_id_type=MESH,
            ).start()

    quarter = shard // 4

    def kind_of(way, base, turn):
        return base + (turn if way == 0 else 1 - turn)

    def arrive(base, turn, step):
        for way in range(2):
            ring_arrival(way, kind_of(way, base, turn), step).wait_recv()

    def advance(event):
        base, turn, step = event
        for way in range(2):
            kind = kind_of(way, base, turn)
            ring_arrival(way, kind, step - 1).wait_recv()
            ring_copy(way, kind, step).start()

    def events(base):
        return [(base, turn, step) for step in range(1, reach) for turn in range(2)][:-1]

    gu_events = events(0)
    d_events = events(2)
    launch_part(0, quarter)

    chunk = length // chunks
    items = [("ow", 0), ("ng", 0)]
    items += [("stream", i) for i in range(chunks)]
    items += [("gated", i) for i in range(chunks)]

    def tp_view(item, slot):
        what, i = item
        if what == "ow":
            return ow_all.at[pl.ds(pl.multiple_of(slot * wide_v, wide_v), wide_v), :]
        if what == "ng":
            return ng_all.at[pl.ds(pl.multiple_of(slot * width, width), width)]
        if what == "stream":
            return stream_all.at[
                pl.ds(i * chunk, chunk), pl.ds(pl.multiple_of(slot * width, width), width)
            ]
        return gated_all.at[
            pl.ds(i * chunk, chunk), pl.ds(pl.multiple_of(slot * wide_v, wide_v), wide_v)
        ]

    def tp_own(item):
        what, i = item
        if what == "ow":
            return ow_ref
        if what == "ng":
            return ng_ref
        if what == "stream":
            return stream_ref.at[pl.ds(i * chunk, chunk), :]
        return tp_view(item, tp)

    def tp_copy(item, route):
        number = items.index(item)
        slot = tp if route < 2 else far
        return pltpu.make_async_remote_copy(
            src_ref=tp_own(item) if route < 2 else tp_view(item, far),
            dst_ref=tp_view(item, slot),
            send_sem=tp_s.at[route, number],
            recv_sem=tp_r.at[route, number],
            device_id=(sp, far if route == 0 else near),
            device_id_type=MESH,
        )

    def tp_arrival(item, route):
        number = items.index(item)
        view = tp_view(item, (far, near, cross)[route])
        return pltpu.make_async_remote_copy(
            src_ref=view,
            dst_ref=view,
            send_sem=tp_s.at[route, number],
            recv_sem=tp_r.at[route, number],
            device_id=(sp, far if route == 0 else near),
            device_id_type=MESH,
        )

    def share(item):
        for route in range(2):
            tp_copy(item, route).start()

    def relay(item):
        tp_arrival(item, 0).wait_recv()
        tp_copy(item, 2).start()

    def settle(item):
        for route in (1, 2):
            tp_arrival(item, route).wait_recv()

    early = items[: 2 + chunks]
    late = items[2 + chunks :]
    for item in early:
        share(item)

    own = [
        pltpu.make_async_copy(g_ref, slot_view(0, sp), local_s.at[0]),
        pltpu.make_async_copy(u_ref, slot_view(1, sp), local_s.at[1]),
        pltpu.make_async_copy(d_ref, wd.at[sp], local_s.at[2]),
        pltpu.make_async_copy(ow_ref, tp_view(("ow", 0), tp), local_s.at[3]),
        pltpu.make_async_copy(
            stream_ref,
            stream_all.at[:, pl.ds(pl.multiple_of(tp * width, width), width)],
            local_s.at[4],
        ),
        pltpu.make_async_copy(ng_ref, tp_view(("ng", 0), tp), local_s.at[5]),
    ]
    for copy in own:
        copy.start()

    both[member] = jnp.zeros(both.shape[1:], jnp.float32)

    for copy in inputs:
        copy.wait()
    for block in range(blocks):
        for unit in range(units):
            spot = block * units + unit
            tokens = slice(block * BLOCK, (block + 1) * BLOCK)
            a_ref[spot : spot + 1, :] = gate_in[unit // heads, unit % heads : unit % heads + 1, tokens]
            b_ref[spot : spot + 1, :] = forget_in[
                unit // heads, unit % heads : unit % heads + 1, tokens
            ]
    raw = b_ref[...]
    forgets = jnp.minimum(raw, 0.0) - jnp.log1p(jnp.exp(-jnp.abs(raw)))
    at_row = lax.broadcasted_iota(jnp.int32, (BLOCK, BLOCK), 0)
    at_col = lax.broadcasted_iota(jnp.int32, (BLOCK, BLOCK), 1)
    upto = (at_row <= at_col).astype(jnp.bfloat16)
    since = (at_row >= at_col).astype(jnp.bfloat16)
    first = forgets.astype(jnp.bfloat16)
    left_over = forgets - first.astype(jnp.float32)
    second = left_over.astype(jnp.bfloat16)
    third = (left_over - second.astype(jnp.float32)).astype(jnp.bfloat16)
    ahead = jnp.zeros_like(forgets)
    behind = jnp.zeros_like(forgets)
    for piece in (third, second, first):
        ahead = ahead + jnp.dot(piece, upto, preferred_element_type=jnp.float32)
        behind = behind + jnp.dot(piece, since, preferred_element_type=jnp.float32)
    spots = lax.broadcasted_iota(jnp.int32, forgets.shape, 0)
    sums = jnp.where(lax.rem(spots, units) < heads, ahead, behind)
    shifted = a_ref[...] - sums
    b_ref[...] = sums
    a_ref[...] = shifted
    total_ref[...] = jnp.broadcast_to(jnp.sum(forgets, axis=1, keepdims=True), forgets.shape)
    peaks = []
    for unit in range(units):
        direction = unit // heads
        beyond = jnp.zeros((1, BLOCK), jnp.float32)
        order = range(blocks - 1, -1, -1) if direction == 0 else range(blocks)
        highest = None
        for block in order:
            spot = block * units + unit
            beyond = beyond + total_ref[spot : spot + 1, :]
            logs = beyond + a_ref[spot : spot + 1, :]
            w_ref[spot : spot + 1, :] = logs
            highest = logs if highest is None else jnp.maximum(highest, logs)
        highest = jnp.broadcast_to(jnp.max(highest, axis=1, keepdims=True), (1, BLOCK))
        peaks.append(highest)
        head = unit % heads
        both[member, direction, head, depth_k + 1 : depth_k + 2, :] = highest
        both[member, direction, head, depth_k + 2 : depth_k + 3, :] = beyond
    for block in range(blocks):
        spot = slice(block * units, (block + 1) * units)
        w_ref[spot, :] = jnp.exp(w_ref[spot, :] - jnp.concatenate(peaks, axis=0))

    lane = lax.broadcasted_iota(jnp.int32, (BLOCK, q_ref.shape[1]), 1)
    lane_row = lax.broadcasted_iota(jnp.int32, (1, q_ref.shape[1]), 1)

    def turn_block(block, normers):
        rows = pl.ds(pl.multiple_of(block * BLOCK, BLOCK), BLOCK)
        spot = pl.ds(block * units, units)
        stacked = jnp.concatenate([b_ref[spot, :], a_ref[spot, :], w_ref[spot, :], w_ref[spot, :]], axis=0)
        columns = stacked.T
        cols_ref[rows, : 4 * units] = columns
        key_wide = k_ref[rows, :].astype(jnp.float32)
        out = []
        for unit in range(units):
            head = unit % heads
            weight = columns[:, 2 * units + unit : 2 * units + unit + 1]
            value = v_ref[rows, head * depth_v : (head + 1) * depth_v].astype(jnp.float32)
            hidden[rows, unit * depth_v : (unit + 1) * depth_v] = (weight * value).astype(jnp.bfloat16)
            out.append(normers[unit] + jnp.sum(weight * key_wide, axis=0, keepdims=True))
        return tuple(out)

    normers = lax.fori_loop(
        0,
        blocks,
        turn_block,
        tuple(jnp.zeros((1, heads * depth_k), jnp.float32) for _ in range(units)),
    )
    outer = lax.dot_general(
        k_ref[...],
        hidden[:, : units * depth_v],
        (((0,), (0,)), ((), ())),
        preferred_element_type=jnp.float32,
    )
    for unit in range(units):
        direction, head = unit // heads, unit % heads
        both[member, direction, head, :depth_k, :] = outer[
            head * depth_k : (head + 1) * depth_k, unit * depth_v : (unit + 1) * depth_v
        ]
        mine = (lane_row >= head * depth_k) & (lane_row < (head + 1) * depth_k)
        both[member, direction, head, depth_k : depth_k + 1, :] = jnp.where(mine, normers[unit], 0.0)

    def mate_copy(which):
        return pltpu.make_async_remote_copy(
            src_ref=both.at[which],
            dst_ref=both.at[which],
            send_sem=mate_s,
            recv_sem=mate_r,
            device_id=(mate, tp),
            device_id_type=MESH,
        )

    def state_copy(k):
        return pltpu.make_async_remote_copy(
            src_ref=pair_sum.at[(pair + k) // pairs],
            dst_ref=others.at[pair],
            send_sem=state_s.at[k],
            recv_sem=state_r.at[k],
            device_id=(2 * lax.rem(pair + k, pairs) + member, tp),
            device_id_type=MESH,
        )

    def state_arrival(k):
        slot = lax.rem(pair - k + pairs, pairs)
        return pltpu.make_async_remote_copy(
            src_ref=others.at[slot],
            dst_ref=others.at[slot],
            send_sem=state_s.at[k],
            recv_sem=state_r.at[k],
            device_id=(2 * slot + member, tp),
            device_id_type=MESH,
        )

    def parts_of(item):
        return (
            item[:depth_k],
            item[depth_k : depth_k + 1],
            item[depth_k + 1 : depth_k + 2],
            item[depth_k + 2 : depth_k + 3],
        )

    def join(earlier, later):
        decayed = earlier[2] + later[3]
        peak = jnp.maximum(decayed, later[2])
        keep = jnp.exp(decayed - peak)
        gain = jnp.exp(later[2] - peak)
        return (
            keep * earlier[0] + gain * later[0],
            keep * earlier[1] + gain * later[1],
            peak,
            earlier[3] + later[3],
        )

    mate_copy(member).start()
    launch_part(quarter, quarter)
    mate_copy(1 - member).wait_recv()
    for direction in range(2):
        for head in range(heads):
            joined = join(
                parts_of(both[direction, direction, head]),
                parts_of(both[1 - direction, direction, head]),
            )
            pair_sum[direction, head, :depth_k, :] = joined[0]
            for i in range(1, 4):
                pair_sum[direction, head, depth_k + i - 1 : depth_k + i, :] = joined[i]
            pair_sum[direction, head, depth_k + 3 :, :] = jnp.zeros((5, depth_v), jnp.float32)

    def send_state(k, carry):
        state_copy(k).start()
        return carry

    lax.fori_loop(1, pairs, send_state, 0)
    launch_part(2 * quarter, shard - 2 * quarter)
    launch(0, 1)

    def wait_state(k, carry):
        state_arrival(k).wait_recv()
        return carry

    lax.fori_loop(1, pairs, wait_state, 0)
    for direction in range(2):
        for head in range(heads):
            unit = direction * heads + head

            def take(j, carry):
                return join(carry, parts_of(others[j if direction == 0 else pairs - 1 - j, head]))

            def take_mate(j, carry):
                return join(carry, parts_of(both[direction, direction, head]))

            zero = jnp.zeros((1, BLOCK), jnp.float32)
            state = (jnp.zeros((depth_k, depth_v), jnp.float32), zero, zero, zero)
            state = lax.fori_loop(0, pair if direction == 0 else pairs - 1 - pair, take, state)
            state = lax.fori_loop(0, member if direction == 0 else 1 - member, take_mate, state)
            c_ref[unit] = jnp.zeros(c_ref.shape[1:], jnp.float32)
            c_ref[unit, head * depth_k : (head + 1) * depth_k, :] = state[0]
            n_ref[unit] = state[1]
            m_ref[unit] = state[2]

    def step(index, carry):
        for direction in range(2):
            block = index if direction == 0 else blocks - 1 - index
            rows = pl.ds(pl.multiple_of(block * BLOCK, BLOCK), BLOCK)
            query = q_ref[rows, :].astype(jnp.float32) * depth_k ** (-0.5)
            key = k_ref[rows, :]
            key_wide = key.astype(jnp.float32)
            cols = cols_ref[rows, :]
            keep = at_col <= at_row if direction == 0 else at_col >= at_row
            for head in range(heads):
                unit = direction * heads + head
                mine = (lane >= head * depth_k) & (lane < (head + 1) * depth_k)
                q_wide = jnp.where(mine, query, 0.0)
                q_own = q_wide.astype(jnp.bfloat16)
                value = v_ref[rows, head * depth_v : (head + 1) * depth_v]
                b_col = cols[:, unit : unit + 1]
                a_col = cols[:, units + unit : units + unit + 1]
                a_row = a_ref[pl.ds(block * units + unit, 1), :]
                total = total_ref[pl.ds(block * units + unit, 1), :]
                m_row = m_ref[unit]
                n_row = n_ref[unit]
                c_state = c_ref[unit]
                decay = jnp.where(keep, b_col + a_row, VERY_LOW)
                carry_log = b_col + m_row[:, :1]
                peak = jnp.maximum(carry_log, jnp.max(decay, axis=1, keepdims=True))
                scores = lax.dot_general(
                    q_own, key, (((1,), (1,)), ((), ())), preferred_element_type=jnp.float32
                ) * jnp.exp(decay - peak)
                carried = jnp.exp(carry_log - peak)
                number = two_pass(scores, value, ((1,), (0,)), True)
                number = number + carried * two_pass(q_own, c_state, ((1,), (0,)), False)
                below = jnp.sum(scores, axis=1, keepdims=True)
                below = below + carried * jnp.sum(q_wide * n_row, axis=1, keepdims=True)
                h_ref[direction, rows, head * depth_v : (head + 1) * depth_v] = number / jnp.maximum(
                    jnp.abs(below), jnp.exp(-peak)
                )
                new_m = jnp.maximum(total + m_row, total + jnp.max(a_row, axis=1, keepdims=True))
                shrink = jnp.exp(total + m_row - new_m)
                weight = jnp.exp(total[:, :1] + a_col - new_m[:, :1])
                weighted = weight * value.astype(jnp.float32)
                c_ref[unit] = shrink[:, :1] * c_state + two_pass(
                    key, weighted, ((0,), (0,)), False
                )
                n_ref[unit] = shrink[:, :1] * n_row + jnp.sum(
                    weight * key_wide, axis=0, keepdims=True
                )
                m_ref[unit] = new_m

        @pl.when(index == (2 * blocks) // 3)
        def _():
            advance(gu_events[0])

        return carry

    lax.fori_loop(0, blocks, step, 0)

    gain = gain_ref[...].astype(jnp.float32).reshape(1, wide_v)

    def finish(index, carry):
        rows = pl.ds(pl.multiple_of(index * BLOCK, BLOCK), BLOCK)
        for head in range(heads):
            span = slice(head * depth_v, (head + 1) * depth_v)
            summed = h_ref[0, rows, span] + h_ref[1, rows, span]
            scale = lax.rsqrt(jnp.mean(summed * summed, axis=1, keepdims=True) + EPSILON)
            opened = 1.0 / (1.0 + jnp.exp(-og_ref[rows, span].astype(jnp.float32)))
            place = pl.multiple_of(tp * wide_v + head * depth_v, depth_v)
            gated_all[rows, pl.ds(place, depth_v)] = (
                summed * scale * gain[:, span] * opened
            ).astype(jnp.bfloat16)
        return carry

    lax.fori_loop(0, blocks, finish, 0)
    for item in late:
        share(item)

    advance(gu_events[1])
    relay(("ow", 0))
    relay(("ng", 0))
    relay(early[2])
    relay(early[3])
    advance(gu_events[2])
    for item in early[4:]:
        relay(item)
    relay(late[0])
    advance(gu_events[3])
    for item in late[1:]:
        relay(item)
    for item in items:
        settle(item)
    for copy in own:
        copy.wait()

    norm_gain = ng_all[...].astype(jnp.float32).reshape(1, features)

    def project(index, carry):
        rows = pl.ds(pl.multiple_of(index * TILE, TILE), TILE)
        total = stream_all[rows, :].astype(jnp.float32) + jnp.dot(
            gated_all[rows, :], ow_all[...], preferred_element_type=jnp.float32
        )
        scale = lax.rsqrt(jnp.mean(total * total, axis=1, keepdims=True) + EPSILON)
        normed[rows, :] = (total * scale * norm_gain).astype(jnp.bfloat16)
        for j in range(features // width):

            @pl.when(tp == j)
            def _():
                res[rows, :] = total[:, j * width : (j + 1) * width]

        @pl.when(index == 2)
        def _():
            advance(gu_events[4])

        return carry

    lax.fori_loop(0, length // TILE, project, 0)
    for event in gu_events[5:]:
        advance(event)
    launch(2, 0)
    launch(2, 1)
    if reach >= 2:
        arrive(0, 1, reach - 2)
    arrive(0, 0, reach - 1)

    slab = 256
    part_rows = length // 2

    def activate(gate, up):
        return (gate / (1.0 + jnp.exp(-gate)) * up).astype(jnp.bfloat16)

    def open_slab(index, carry):
        first = pl.multiple_of(index * slab, slab)
        gate_cut = wgu[:, :, pl.ds(first, slab)].reshape(features, slab)
        up_cut = wgu[:, :, pl.ds(pl.multiple_of(hw + index * slab, BLOCK), slab)].reshape(
            features, slab
        )
        for part in range(2):
            rows = slice(part * part_rows, (part + 1) * part_rows)
            gate = jnp.dot(normed[rows, :], gate_cut, preferred_element_type=jnp.float32)
            up = jnp.dot(normed[rows, :], up_cut, preferred_element_type=jnp.float32)
            hidden[rows, pl.ds(first, slab)] = activate(gate, up)
        for at_slab, number in ((2, 0), (4, 1)):

            @pl.when(index == at_slab)
            def _():
                advance(d_events[number])

        return carry

    slabs = hw // slab
    lax.fori_loop(0, slabs, open_slab, 0)
    rest = hw - slabs * slab
    if rest:
        cut = jnp.concatenate(
            [wgu[:, :, slabs * slab : hw], wgu[:, :, hw + slabs * slab :]], axis=2
        ).reshape(features, 2 * rest)
        for part in range(2):
            rows = slice(part * part_rows, (part + 1) * part_rows)
            last = jnp.dot(normed[rows, :], cut, preferred_element_type=jnp.float32)
            hidden[rows, slabs * slab :] = activate(last[:, :rest], last[:, rest:])

    per_owner = width // PIECE
    by_arrival = shard == 2 * PIECE and per_owner == 4

    def stage(slot):
        return normed.at[:, pl.ds(pl.multiple_of(slot * PIECE, PIECE), PIECE)]

    def a_copy(slot):
        return pltpu.make_async_remote_copy(
            src_ref=stage(slot),
            dst_ref=recv_a.at[slot],
            send_sem=a_s.at[slot],
            recv_sem=a_r.at[slot],
            device_id=(sp, near),
            device_id_type=MESH,
        )

    def x_copy(slot):
        return pltpu.make_async_remote_copy(
            src_ref=stage(2 * per_owner + slot),
            dst_ref=recv_x.at[slot],
            send_sem=x_s.at[slot],
            recv_sem=x_r.at[slot],
            device_id=(sp, far),
            device_id_type=MESH,
        )

    if not by_arrival:
        for event in d_events[2:]:
            advance(event)
        arrive(2, 1, reach - 2)
        arrive(2, 0, reach - 1)

    def lower(index, carry):
        if by_arrival:
            hop = ((index + 1) // 2) * (1 - 2 * lax.rem(index, 2))
            sources = (at(pos + hop), at(pos - hop))
            for event in d_events[2:]:

                @pl.when(index == 2 * event[2] - 1 + event[1])
                def _():
                    advance(event)

            @pl.when(index == 2 * reach - 2)
            def _():
                arrive(2, 1, reach - 2)

            @pl.when(index == 2 * reach - 1)
            def _():
                arrive(2, 0, reach - 1)

            cut = jnp.concatenate([wd[sources[0], :PIECE, :], wd[sources[1], PIECE:, :]], axis=0)
            pieces = (2 * sources[0], 2 * sources[1] + 1)
        else:
            group = 2 * PIECE // shard
            cut = wd[pl.ds(pl.multiple_of(index * group, group), group)].reshape(2 * PIECE, hw)
            pieces = (2 * index, 2 * index + 1)
        product = lax.dot_general(
            hidden[...], cut, (((1,), (1,)), ((), ())), preferred_element_type=jnp.float32
        )
        parts = (product[:, :PIECE], product[:, PIECE:])
        roles = []
        for piece in pieces:
            owner = piece // per_owner
            low = lax.rem(lax.rem(tp, 2) + lax.rem(owner, 2), 2)
            high = lax.rem(tp // 2 + owner // 2, 2)
            roles.append((low, high, lax.rem(piece, per_owner)))

        for part, (low, high, slot) in zip(parts, roles):

            @pl.when(low == 1)
            def _():
                place = high * per_owner + slot
                first = pl.multiple_of(place * PIECE, PIECE)
                normed[:, pl.ds(first, PIECE)] = part.astype(jnp.bfloat16)
                a_copy(place).start()

        for part, (low, high, slot) in zip(parts, roles):

            @pl.when((low == 0) & (high == 0))
            def _():
                first = pl.multiple_of(slot * PIECE, PIECE)
                res[:, pl.ds(first, PIECE)] = res[:, pl.ds(first, PIECE)] + part

        for part, (low, high, slot) in zip(parts, roles):

            @pl.when((low == 0) & (high == 1))
            def _():
                a_copy(per_owner + slot).wait_recv()
                first = pl.multiple_of((2 * per_owner + slot) * PIECE, PIECE)
                normed[:, pl.ds(first, PIECE)] = (
                    part + recv_a[per_owner + slot].astype(jnp.float32)
                ).astype(jnp.bfloat16)
                x_copy(slot).start()

        return carry

    lax.fori_loop(0, features // (2 * PIECE), lower, 0)

    for turn in range(per_owner):
        if by_arrival:
            hops_even = lax.rem(pos - tp + n, n)
            hops_odd = lax.rem(pos + 1 + tp, n)
            far_even = reach - jnp.abs(reach - hops_even)
            far_odd = reach - jnp.abs(reach - hops_odd)
            late = (far_even > far_odd).astype(jnp.int32)
            side = late + (turn // 2) * (1 - 2 * late)
            slot = 2 * side + turn % 2
        else:
            slot = turn
        a_copy(slot).wait_recv()
        x_copy(slot).wait_recv()
        span = pl.ds(pl.multiple_of(slot * PIECE, PIECE), PIECE)
        out_ref[:, span] = (
            res[:, span] + recv_a[slot].astype(jnp.float32) + recv_x[slot].astype(jnp.float32)
        ).astype(jnp.bfloat16)

    def state_left(k, carry):
        state_copy(k).wait_send()
        return carry

    lax.fori_loop(1, pairs, state_left, 0)
    mate_copy(member).wait_send()
    for base in (0, 2):
        for way in range(2):
            for turn in range(2):
                ring_copy(way, kind_of(way, base, turn), 0).wait_send()
        for _, turn, hop in events(base):
            for way in range(2):
                ring_copy(way, kind_of(way, base, turn), hop).wait_send()
    for item in items:
        for route in range(3):
            tp_copy(item, route).wait_send()
    for slot in range(2 * per_owner):
        a_copy(slot).wait_send()
    for slot in range(per_owner):
        x_copy(slot).wait_send()


def local(
    query,
    key_rows,
    value,
    in_gate,
    forget_pre,
    out_gate,
    head_gain,
    out_weight,
    stream,
    norm_gain,
    gate_weight,
    up_weight,
    down_weight,
):
    length = query.shape[0]
    heads = in_gate.shape[1]
    depth_k = query.shape[1] // heads
    depth_v = value.shape[1] // heads
    blocks = length // BLOCK
    n_sp = lax.axis_size("sp")
    n_tp = lax.axis_size("tp")
    assert n_tp == 4 and n_sp % 2 == 0
    width = stream.shape[1]
    features = width * n_tp
    shard, hidden_width = gate_weight.shape
    units = 2 * heads
    chunks = next(c for c in (3, 2, 1) if blocks % c == 0)
    per_owner = width // PIECE
    reach = n_sp // 2
    wide_v = heads * depth_v
    dma = pltpu.SemaphoreType.DMA
    bf16, f32 = jnp.bfloat16, jnp.float32
    vmem = pl.BlockSpec(memory_space=pltpu.VMEM)
    anywhere = pl.BlockSpec(memory_space=pl.ANY)
    return pl.pallas_call(
        functools.partial(layer_kernel, n_sp, heads, chunks),
        out_shape=pltpu.VMEM((length, width), bf16),
        in_specs=[vmem] * 3 + [anywhere] * 10,
        out_specs=vmem,
        scratch_shapes=[
            pltpu.VMEM(query.shape, bf16),
            pltpu.VMEM(key_rows.shape, bf16),
            pltpu.VMEM(value.shape, bf16),
            pltpu.VMEM(out_gate.shape, bf16),
            pltpu.VMEM((blocks * units, BLOCK), f32),
            pltpu.VMEM((blocks * units, BLOCK), f32),
            pltpu.VMEM((blocks * units, BLOCK), f32),
            pltpu.VMEM((blocks * units, BLOCK), f32),
            pltpu.VMEM((length, 4 * units), f32),
            pltpu.VMEM((2, 2, heads, depth_k + 8, depth_v), f32),
            pltpu.VMEM((2, heads, depth_k + 8, depth_v), f32),
            pltpu.VMEM((n_sp, shard, 2 * hidden_width), bf16),
            pltpu.VMEM((n_sp, shard, hidden_width), bf16),
            pltpu.VMEM((n_tp * wide_v, features), bf16),
            pltpu.VMEM((length, features), bf16),
            pltpu.VMEM((length, n_tp * wide_v), bf16),
            pltpu.VMEM((features,), bf16),
            pltpu.VMEM((length, features), bf16),
            pltpu.VMEM((length, hidden_width), bf16),
            pltpu.VMEM((length, width), f32),
            pltpu.VMEM((2, length, wide_v), f32),
            pltpu.VMEM((units, heads * depth_k, depth_v), f32),
            pltpu.VMEM((units, 1, heads * depth_k), f32),
            pltpu.VMEM((units, 1, BLOCK), f32),
            pltpu.VMEM((n_sp // 2, heads, depth_k + 8, depth_v), f32),
            pltpu.VMEM((2 * per_owner, length, PIECE), bf16),
            pltpu.VMEM((per_owner, length, PIECE), bf16),
            dma((2, 4, reach)),
            dma((2, 4, reach)),
            dma,
            dma,
            dma((n_sp // 2,)),
            dma((n_sp // 2,)),
            dma((3, 2 + 2 * chunks)),
            dma((3, 2 + 2 * chunks)),
            dma((2 * per_owner,)),
            dma((2 * per_owner,)),
            dma((per_owner,)),
            dma((per_owner,)),
            dma((10,)),
        ],
        compiler_params=pltpu.CompilerParams(
            collective_id=0, has_side_effects=True, vmem_limit_bytes=65_000_000
        ),
        name="layer",
    )(
        in_gate,
        forget_pre,
        head_gain,
        query,
        key_rows,
        value,
        out_gate,
        norm_gain,
        stream,
        out_weight,
        gate_weight,
        up_weight,
        down_weight,
    )


def solution(mesh):
    placed = (
        P("sp", "tp"),
        P("sp", "tp"),
        P("sp", "tp"),
        P(None, "tp", "sp"),
        P(None, "tp", "sp"),
        P("sp", "tp"),
        P("tp"),
        P("tp", None),
        P("sp", "tp"),
        P("tp"),
        P("sp", "tp"),
        P("sp", "tp"),
        P("sp", "tp"),
    )
    return jax.shard_map(
        local, mesh=mesh, in_specs=placed, out_specs=P("sp", "tp"), check_vma=False
    )
```
